128 devices in a mesh: sp: 32 (over z, y, core), tp: 4 (over x).
Axes of the slice: x: 4, y: 4, z: 4, core: 2. Of those that a mesh axis runs over, the one named last changes fastest.
Arguments:
- tokens: bfloat16 [4096, 6, 2048], P(('sp', 'tp')), may hold values from -6 to 6
- norm_gain: float32 [2048], replicated, may hold values from 0.1 to 1.9
- w_query: bfloat16 [3, 2048, 1024], P(None, 'sp', 'tp'), may hold values from -0.125 to 0.125
- w_key: bfloat16 [3, 2048, 1024], P(None, 'sp', 'tp'), may hold values from -0.125 to 0.125
- w_value: bfloat16 [3, 2048, 1024], P(None, 'sp', 'tp'), may hold values from -0.125 to 0.125
- w_out: bfloat16 [1024, 2048], P('tp', 'sp'), may hold values from -0.1875 to 0.1875
Outputs:
- mixed: bfloat16 [4096, 6, 2048], P(('sp', 'tp'))
- log_weight: float32 [4096, 6, 8], P('sp', None, 'tp')
The draws below stay inside these ranges and needn't reach their ends.
All inputs are finite; a program needn't handle non-finite values.
Results may differ from the reference program's by a relative error of at most 0.015.
Values may be sent and summed in bfloat16 or wider, within the bound.
A program may use at most 128 MiB of HBM per device.

```python
import jax
import jax.numpy as jnp
from jax import lax

WIDTH = 2048
GROUPS = 3
HEADS = 8
HEAD_WIDTH = 128
STEPS = 24
DILATION_MIDDLE = 4
DILATION_WIDE = 16
BATCH = 6
LENGTH = 4096


def shard_levels(own_key, dims, pieces, least, high):
    def one(dim, blocks):
        draws = jax.random.uniform(jax.random.fold_in(jax.random.fold_in(own_key, 6), dim), (blocks,), jnp.float32, least / len(pieces), high / len(pieces))
        return jnp.repeat(jnp.exp(draws), dims[dim] // blocks).reshape((-1,) + (1,) * (len(dims) - dim - 1))

    factor_of = one(*pieces[0])
    for cut in pieces[1:]:
        factor_of = factor_of * one(*cut)
    return factor_of


def normal_values(rng, dims, spread, limit, cuts=(), kind=jnp.bfloat16):
    array = jax.random.normal(rng, dims, jnp.float32) * spread
    if len(cuts) > 0:
        array = shard_levels(rng, dims, cuts, -0.22, 0.18) * array
    return jnp.clip(array, min=-limit, max=limit).astype(kind)


def setup_inputs(seed: int = 0) -> dict:
    splits = jax.random.split(jax.random.key(seed), 7)
    tokens = normal_values(splits[0], (LENGTH, BATCH, WIDTH), 1.0, 6.0, ((0, 128),))
    norm_gain = jnp.clip(1.0 + 0.18 * jax.random.normal(splits[1], (WIDTH,), jnp.float32), 0.1, 1.9)
    w_query = normal_values(splits[2], (GROUPS, WIDTH, HEADS * HEAD_WIDTH), WIDTH ** -0.5, 0.125, ((1, 32), (2, 4)))
    w_key = normal_values(splits[3], (GROUPS, WIDTH, HEADS * HEAD_WIDTH), WIDTH ** -0.5, 0.125, ((1, 32), (2, 4)))
    w_value = normal_values(splits[4], (GROUPS, WIDTH, HEADS * HEAD_WIDTH), WIDTH ** -0.5, 0.125, ((1, 32), (2, 4)))
    w_out = normal_values(splits[5], (HEADS * HEAD_WIDTH, WIDTH), (HEADS * HEAD_WIDTH) ** -0.5, 0.1875, ((0, 4), (1, 32)))
    return dict(tokens=tokens, norm_gain=norm_gain, w_query=w_query, w_key=w_key, w_value=w_value, w_out=w_out)


epsilon = 1e-06

def rms_normed(values, gain):
    widened = values.astype(jnp.float32)
    scaled = widened * lax.rsqrt(lax.optimization_barrier(jnp.mean(widened * widened, axis=-1, keepdims=True)) + epsilon)
    return (scaled * gain.astype(jnp.float32)).astype(jnp.bfloat16)

def reference(tokens, norm_gain, w_query, w_key, w_value, w_out):
    seq_count, batch_count, width_count = tokens.shape
    normed = rms_normed(tokens, norm_gain)
    flat_rows = normed.reshape(seq_count * batch_count, width_count)
    positions = jnp.arange(seq_count, dtype=jnp.int32)
    scale = 1.0 / HEAD_WIDTH ** 0.5
    group_logs = []
    group_outs = []
    for group_index, dilation in enumerate((1, DILATION_MIDDLE, DILATION_WIDE)):

        def project(weight):
            product = jnp.dot(flat_rows, weight[group_index], preferred_element_type=jnp.float32)
            return product.astype(jnp.bfloat16).reshape(seq_count, batch_count, HEADS, HEAD_WIDTH).astype(jnp.float32)
        queries = project(w_query)
        keys = project(w_key)
        values = project(w_value)
        score_list = []
        for lag_index in range(STEPS + 1):
            offset = lag_index * dilation
            moved = jnp.pad(keys, ((offset, 0), (0, 0), (0, 0), (0, 0)))[:seq_count]
            score = jnp.einsum('sbhe,sbhe->sbh', queries, moved, precision=lax.Precision.HIGHEST) * scale
            score_list.append(jnp.where((positions >= offset)[:, None, None], score, jnp.float32(-1e+30)))
        scores = jnp.stack(score_list)
        peak = lax.optimization_barrier(jnp.max(scores, axis=0))
        lifted = jnp.exp(scores - peak[None])
        totals = lax.optimization_barrier(jnp.sum(lifted, axis=0))
        group_logs.append(peak + jnp.log(totals))
        probs = (lifted / totals[None]).astype(jnp.bfloat16).astype(jnp.float32)
        accumulated = jnp.zeros((seq_count, batch_count, HEADS, HEAD_WIDTH), jnp.float32)
        for lag_index in range(STEPS + 1):
            offset = lag_index * dilation
            moved = jnp.pad(values, ((offset, 0), (0, 0), (0, 0), (0, 0)))[:seq_count]
            accumulated = accumulated + probs[lag_index][..., None] * moved
        group_outs.append(accumulated.astype(jnp.bfloat16))
    stacked_logs = jnp.stack(group_logs)
    top_log = lax.optimization_barrier(jnp.max(stacked_logs, axis=0))
    log_weight = top_log + jnp.log(lax.optimization_barrier(jnp.sum(jnp.exp(stacked_logs - top_log[None]), axis=0)))
    shares = jax.nn.softmax(stacked_logs, axis=0)
    outputs = jnp.stack(group_outs).astype(jnp.float32)
    combined = lax.optimization_barrier(jnp.sum(shares[..., None] * outputs, axis=0)).astype(jnp.bfloat16)
    combined = combined.reshape(seq_count * batch_count, HEADS * HEAD_WIDTH)
    mixed = jnp.dot(combined, w_out, preferred_element_type=jnp.float32).astype(jnp.bfloat16)
    return (mixed.reshape(seq_count, batch_count, width_count), log_weight)
```

```python
import functools
import math

import jax
import jax.numpy as jnp
from jax import lax
from jax.experimental import pallas as pl
from jax.experimental.pallas import tpu as pltpu
from jax.sharding import PartitionSpec as P

MESH = pl.DeviceIdType.MESH
BATCH = 6
WIDTH = 2048
HEAD = 128
STEPS = 24
EPSILON = 1e-06
ROWS = 256
PIECE = 32
HALO = (32, 96, 384)
SPAN = (160, 224, 512)
DILATION = (1, 4, 16)
COPIES = 160
F32 = jnp.float32
BF16 = jnp.bfloat16
NT = (((1,), (1,)), ((), ()))
TN = (((0,), (0,)), ((), ()))


class Sender:
    def __init__(self, send_sem, recv_sem):
        self.send_sem, self.recv_sem, self.started = send_sem, recv_sem, []

    def __call__(self, src, dst, device):
        slot = len(self.started)
        copy = pltpu.make_async_remote_copy(
            src_ref=src,
            dst_ref=dst,
            send_sem=self.send_sem.at[slot],
            recv_sem=self.recv_sem.at[slot],
            device_id=device,
            device_id_type=MESH,
        )
        copy.start()
        self.started.append(copy)
        return copy


class PlaneGather:
    def __init__(self, send, block, a, b, to_a, to_b):
        self.send, self.block, self.a, self.b = send, block, a, b
        self.to_a, self.to_b = to_a, to_b
        self.across = {}

    def put(self, da, db, device, half=None):
        ref = self.block((self.a + da + 4) % 4, (self.b + db + 4) % 4, half)
        return self.send(ref, ref, device)

    def spread(self, da):
        for side in (1, -1):
            self.across[da, side] = self.put(da, 0, self.to_b[side])

    def begin(self):
        self.along = {side: self.put(0, 0, self.to_a[side]) for side in (1, -1)}
        self.spread(0)

    def first(self):
        self.far = {}
        for side, half in ((1, 0), (-1, 1)):
            self.along[side].wait_recv()
            self.far[side] = self.put(-side, 0, self.to_a[side], half)
            self.spread(-side)

    def second(self):
        for side in (1, -1):
            self.far[side].wait_recv()
        self.spread(2)

    def third(self):
        self.last = []
        for da, side in ((0, 1), (-1, -1), (1, 1), (2, -1)):
            self.across[da, side].wait_recv()
            self.last.append(self.put(da, -side, self.to_b[side]))

    def finish(self):
        for da, side in ((0, -1), (-1, 1), (1, -1), (2, 1)):
            self.across[da, side].wait_recv()
        for copy in self.last:
            copy.wait_recv()


def kernel(
    tokens_ref, gain_ref, wq_ref, wk_ref, wv_ref, wo_ref,
    mixed_ref, logs_ref,
    raw, normed, weights, w_out, queries, kv0, kv1, kv2, bias, heads, gathered,
    own_logs, partner_logs, send_sem, recv_sem, local_sem,
):
    s, x = lax.axis_index("sp"), lax.axis_index("tp")
    c, q = s % 2, s // 2
    y, z = q % 4, q // 4
    kv = (kv0, kv1, kv2)
    send = Sender(send_sem, recv_sem)

    def at(chip, core, column):
        return (chip * 2 + core, column)

    def chip_of(a, b):
        return (1 - c) * (b * 4 + a) + c * (a * 4 + b)

    a, b = (1 - c) * y + c * z, (1 - c) * z + c * y
    to_a = {d: at(chip_of((a + d + 4) % 4, b), c, x) for d in (1, -1)}
    to_b = {d: at(chip_of(a, (b + d + 4) % 4), c, x) for d in (1, -1)}
    xs = {d: (x + d + 4) % 4 for d in (1, -1, 2)}
    to_x = {d: at(q, c, xs[d]) for d in (1, -1, 2)}
    partner = at(q, 1 - c, x)
    onward, behind = at((q + 1) % 16, c, x), at((q + 15) % 16, c, x)

    def local(src, dst, slot):
        copy = pltpu.make_async_copy(src, dst, local_sem.at[slot])
        copy.start()
        return copy

    load = local(tokens_ref, raw, 0)
    mine = pl.ds(pl.multiple_of(q * 128 + c * 64, 64), 64)
    roles = (wk_ref, wv_ref, wq_ref)
    own_columns = pl.ds(pl.multiple_of(c * HEAD, HEAD), HEAD)
    other_columns = pl.ds(pl.multiple_of((1 - c) * HEAD, HEAD), HEAD)
    kept = {}
    for g in (2, 1, 0):
        for r, ref in enumerate(roles):
            kept[g, r] = local(
                ref.at[g, :, own_columns],
                weights.at[g, mine, pl.ds(r * HEAD, HEAD)],
                1 + g * 3 + r,
            )
    x_columns = {d: pl.ds(pl.multiple_of(((x + d + 4) % 4) * 256, 256), 256) for d in (0, 1, -1, 2)}
    kept_out = local(wo_ref, w_out.at[q, c, :, x_columns[0]], 10)

    barrier = pltpu.get_barrier_semaphore()
    peers = [partner, to_a[1], to_a[-1], to_b[1], to_b[-1], onward, behind]
    for d in (1, -1, 2):
        peers += [at(q, c, xs[d]), at(q, 1 - c, xs[d])]
    for peer in peers:
        pl.semaphore_signal(barrier, inc=1, device_id=peer, device_id_type=MESH)
    pl.semaphore_wait(barrier, len(peers))

    swapped = {}
    for g in (2, 1, 0):
        for r, ref in enumerate(roles):
            swapped[g, r] = send(
                ref.at[g, :, other_columns],
                weights.at[g, mine, pl.ds(r * HEAD, HEAD)],
                partner,
            )

    def slab(core, column):
        return pl.ds(pl.multiple_of(core * 128 + column * PIECE, PIECE), PIECE)

    load.wait()
    own_slab = slab(c, x)

    def norm_one(i, _):
        wide = raw[i].astype(F32)
        mean = jnp.sum(wide * wide, axis=-1, keepdims=True) * (1.0 / WIDTH)
        scaled = wide * lax.rsqrt(mean + EPSILON)
        normed[i, own_slab, :] = (scaled * gain_ref[...]).astype(BF16)
        return 0

    lax.fori_loop(0, BATCH, norm_one, 0)

    halves = (pl.ds(0, 3), pl.ds(3, 3))

    def tokens_of(half, column):
        return normed.at[halves[half], slab(c, column), :]

    ring, mirrored = {}, []
    for step in range(2):
        for side in (1, -1):
            half = step if side == 1 else 1 - step
            ref = tokens_of(half, x)
            ring[side, half] = send(ref, ref, to_x[side])
        ref = tokens_of(step, x)
        mirrored.append(send(ref, ref, partner))

    def mirror(half, column):
        ref = tokens_of(half, column)
        copy = send(ref, ref, partner)
        mirrored.append(copy)
        return copy

    def block_of(g):
        def block(ba, bb, half):
            row = chip_of(ba, bb) * 128
            if half is None:
                return weights.at[g, pl.ds(pl.multiple_of(row, 128), 128), :]
            return weights.at[g, pl.ds(pl.multiple_of(row + 64 * half, 64), 64), :]

        return block

    def out_block(ba, bb, half):
        chip = chip_of(ba, bb)
        if half is None:
            return w_out.at[chip, c, :, x_columns[0]]
        return w_out.at[chip, c, pl.ds(32 * half, 32), x_columns[0]]

    plane = [PlaneGather(send, block_of(g), a, b, to_a, to_b) for g in range(3)]
    plane_out = PlaneGather(send, out_block, a, b, to_a, to_b)

    def begin(g):
        for r in range(3):
            kept[g, r].wait()
            swapped[g, r].wait_recv()
        plane[g].begin()

    def project(g, deltas):
        def one(i, _):
            core = i % 2
            column = (x + deltas[0] + i // 2 + 4) % 4
            rows = normed[:, slab(core, column), :].reshape(BATCH * PIECE, WIDTH)
            product = jnp.dot(rows, weights[g], preferred_element_type=F32).astype(BF16)
            product = product.reshape(BATCH, PIECE, 3 * HEAD)
            start = core * 128 + column * PIECE
            kv[g][:, pl.ds(pl.multiple_of(HALO[g] + start, PIECE), PIECE), :] = product[:, :, : 2 * HEAD]
            queries[g, :, pl.ds(pl.multiple_of(start, PIECE), PIECE), :] = product[:, :, 2 * HEAD :]
            return 0

        lax.fori_loop(0, 2 * len(deltas), one, 0)

    wide_sent = {}

    def send_wide(d):
        column = (x + d + 4) % 4
        for core in (1, 0):
            start = core * 128 + column * PIECE
            wide_sent[core, d] = send(
                kv2.at[:, pl.ds(pl.multiple_of(384 + start, PIECE), PIECE), :],
                kv2.at[:, pl.ds(pl.multiple_of(128 + start, PIECE), PIECE), :],
                onward,
            )

    def forward_wide(d):
        column = (x + d + 4) % 4
        wide_sent[1, d].wait_recv()
        return send(
            kv2.at[:, pl.ds(pl.multiple_of(256 + column * PIECE, PIECE), PIECE), :],
            kv2.at[:, pl.ds(pl.multiple_of(column * PIECE, PIECE), PIECE), :],
            onward,
        )

    begin(2)
    plane[2].first()
    begin(1)
    plane[2].second()
    plane[2].third()
    plane[1].first()

    own_logs[...] = jnp.zeros_like(own_logs)

    for half in range(2):
        row = 0
        for g in (2, 1, 0):
            key = lax.broadcasted_iota(jnp.int32, (SPAN[g], 128), 0)
            lane = lax.broadcasted_iota(jnp.int32, (SPAN[g], 128), 1)
            lag = lane - key + HALO[g]
            position = key + (half * 128 - HALO[g]) + q * ROWS
            seen = (lag >= 0) & (lag <= STEPS * DILATION[g]) & (position >= 0)
            if DILATION[g] > 1:
                seen = seen & ((lag & (DILATION[g] - 1)) == 0)
            bias[half, row : row + SPAN[g], :] = jnp.where(seen, F32(0), F32(-1e30))
            row += SPAN[g]

    ring[1, 0].wait_recv()
    far = {1: send(tokens_of(0, xs[-1]), tokens_of(0, xs[-1]), to_x[1])}
    mirror(0, xs[-1])
    ring[-1, 1].wait_recv()
    far[-1] = send(tokens_of(1, xs[1]), tokens_of(1, xs[1]), to_x[-1])
    mirror(1, xs[1])
    plane[2].finish()
    begin(0)
    for copy in mirrored[:2]:
        copy.wait_recv()
    project(2, (0,))
    send_wide(0)
    plane[1].second()
    plane[1].third()
    plane[0].first()
    kept_out.wait()
    plane_out.begin()
    ring[1, 1].wait_recv()
    mirror(1, xs[-1])
    ring[-1, 0].wait_recv()
    mirror(0, xs[1])
    plane[1].finish()
    for copy in mirrored[2:6]:
        copy.wait_recv()
    project(2, (1,))
    send_wide(1)
    project(2, (-1,))
    send_wide(-1)
    plane[0].second()
    project(1, (-1, 0, 1))
    plane[0].third()
    plane_out.first()
    plane_out.second()
    plane_out.third()
    far[1].wait_recv()
    mirror(0, xs[2])
    far[-1].wait_recv()
    mirror(1, xs[2])
    for copy in mirrored[6:]:
        copy.wait_recv()
    project(2, (2,))
    send_wide(2)
    project(1, (2,))
    middle = send(kv1.at[:, pl.ds(ROWS, 96), :], kv1.at[:, pl.ds(0, 96), :], onward)
    plane_out.finish()
    out_halves = (pl.ds(0, 8), pl.ds(8, 8))

    def out_of(half, d):
        return w_out.at[out_halves[half], c, :, x_columns[d]]

    out_ring = {}
    for step in range(2):
        for side in (1, -1):
            half = step if side == 1 else 1 - step
            out_ring[side, half] = send(out_of(half, 0), out_of(half, 0), to_x[side])
    out_mirror = []

    def mirror_out(d):
        ref = w_out.at[:, c, :, x_columns[d]]
        out_mirror.append(send(ref, ref, partner))

    mirror_out(0)
    plane[0].finish()
    project(0, (-1, 0, 1, 2))
    near = send(kv0.at[:, pl.ds(ROWS, 32), :], kv0.at[:, pl.ds(0, 32), :], onward)
    late = [forward_wide(d) for d in (0, 1, -1, 2)]
    out_far = {}
    for side, half in ((1, 0), (-1, 1)):
        out_ring[side, half].wait_recv()
        out_far[side] = send(out_of(half, -side), out_of(half, -side), to_x[side])
    for side, half in ((1, 1), (-1, 0)):
        out_ring[side, half].wait_recv()
        mirror_out(-side)
    for d in (0, 1, -1, 2):
        wide_sent[0, d].wait_recv()
    middle.wait_recv()
    near.wait_recv()
    for copy in late:
        copy.wait_recv()

    scale = 1.0 / math.sqrt(HEAD)
    column_of_mine = pl.ds(pl.multiple_of((2 * x + c) * HEAD, HEAD), HEAD)
    for half in range(2):

        def attend(i, _):
            parts, row = [], 0
            for g in (2, 1, 0):
                keys = kv[g][i, pl.ds(half * 128, SPAN[g]), pl.ds(0, HEAD)]
                query = queries[g, i, pl.ds(half * 128, 128), :]
                score = lax.dot_general(keys, query, NT, preferred_element_type=F32)
                parts.append(score * scale + bias[half, row : row + SPAN[g], :])
                row += SPAN[g]
            peak = functools.reduce(jnp.maximum, [jnp.max(p, axis=0, keepdims=True) for p in parts])
            total = jnp.zeros((1, 128), F32)
            mixture = jnp.zeros((HEAD, 128), F32)
            for g, part in zip((2, 1, 0), parts):
                lifted = jnp.exp(part - peak)
                total = total + jnp.sum(lifted, axis=0, keepdims=True)
                values = kv[g][i, pl.ds(half * 128, SPAN[g]), pl.ds(HEAD, HEAD)]
                mixture = mixture + lax.dot_general(
                    values, lifted.astype(BF16), TN, preferred_element_type=F32
                )
            own_logs[half, pl.ds(i, 1), :] = peak + jnp.log(total)
            heads[i, pl.ds(half * 128, 128), :] = (mixture / total).T.astype(BF16)
            return 0

        lax.fori_loop(0, BATCH, attend, 0)
        if half == 1:
            logs_copy = send(own_logs.at[1 - c], partner_logs, partner)
            copies = []
            for d in (2, 1, -1):
                for core in (c, 1 - c):
                    copies.append(
                        send(
                            heads.at[:, slab(core, xs[d]), :],
                            gathered.at[:, :, column_of_mine],
                            at(q, core, xs[d]),
                        )
                    )
            copies.append(
                send(heads.at[:, slab(1 - c, x), :], gathered.at[:, :, column_of_mine], partner)
            )
            stay = local(heads.at[:, slab(c, x), :], gathered.at[:, :, column_of_mine], 11)
    for side in (1, -1):
        out_far[side].wait_recv()
    mirror_out(2)
    logs_copy.wait_recv()
    mine_logs, their_logs = own_logs[c], partner_logs[...]
    first = jnp.where(c == 0, mine_logs, their_logs)
    second = jnp.where(c == 0, their_logs, mine_logs)
    logs_ref[:, 0, :] = first[:BATCH]
    logs_ref[:, 1, :] = second[:BATCH]
    for copy in copies:
        copy.wait_recv()
    stay.wait()
    for copy in out_mirror:
        copy.wait_recv()

    combined = gathered[...].reshape(BATCH * PIECE, 8 * HEAD)

    def out_tile(i, _):
        tile = w_out[pl.ds(i * 4, 4)].reshape(512, 8 * HEAD)
        product = lax.dot_general(combined, tile, NT, preferred_element_type=F32)
        columns = pl.ds(pl.multiple_of(i * 512, 512), 512)
        mixed_ref[:, :, columns] = product.astype(BF16).reshape(BATCH, PIECE, 512)
        return 0

    lax.fori_loop(0, 4, out_tile, 0)
    for copy in send.started:
        copy.wait_send()


def layer(tokens, norm_gain, w_query, w_key, w_value, w_out):
    any_space = pl.BlockSpec(memory_space=pl.ANY)
    vmem = pl.BlockSpec(memory_space=pltpu.VMEM)
    mixed, logs = pl.pallas_call(
        kernel,
        out_shape=(
            jax.ShapeDtypeStruct((BATCH, PIECE, WIDTH), BF16),
            jax.ShapeDtypeStruct((BATCH, 2, 128), F32),
        ),
        in_specs=[any_space, vmem, any_space, any_space, any_space, any_space],
        out_specs=(vmem, vmem),
        scratch_shapes=[
            pltpu.VMEM((BATCH, PIECE, WIDTH), BF16),
            pltpu.VMEM((BATCH, ROWS, WIDTH), BF16),
            pltpu.VMEM((3, WIDTH, 3 * HEAD), BF16),
            pltpu.VMEM((16, 2, 64, 8 * HEAD), BF16),
            pltpu.VMEM((3, BATCH, ROWS, HEAD), BF16),
            pltpu.VMEM((BATCH, HALO[0] + ROWS, 2 * HEAD), BF16),
            pltpu.VMEM((BATCH, HALO[1] + ROWS, 2 * HEAD), BF16),
            pltpu.VMEM((BATCH, HALO[2] + ROWS, 2 * HEAD), BF16),
            pltpu.VMEM((2, sum(SPAN), 128), F32),
            pltpu.VMEM((BATCH, ROWS, HEAD), BF16),
            pltpu.VMEM((BATCH, PIECE, 8 * HEAD), BF16),
            pltpu.VMEM((2, 8, 128), F32),
            pltpu.VMEM((8, 128), F32),
            pltpu.SemaphoreType.DMA((COPIES,)),
            pltpu.SemaphoreType.DMA((COPIES,)),
            pltpu.SemaphoreType.DMA((12,)),
        ],
        compiler_params=pltpu.CompilerParams(
            collective_id=0, has_side_effects=True, vmem_limit_bytes=56 * 1024 * 1024
        ),
    )(
        jnp.transpose(tokens, (1, 0, 2)),
        norm_gain.reshape(1, WIDTH),
        w_query,
        w_key,
        w_value,
        jnp.transpose(w_out),
    )
    return jnp.transpose(mixed, (1, 0, 2)), jnp.transpose(logs, (2, 0, 1))


def solution(mesh):
    in_specs = (
        P(("sp", "tp"), None, None),
        P(),
        P(None, "sp", "tp"),
        P(None, "sp", "tp"),
        P(None, "sp", "tp"),
        P("tp", "sp"),
    )
    out_specs = (P(("sp", "tp"), None, None), P("sp", None, "tp"))
    return jax.shard_map(layer, mesh=mesh, in_specs=in_specs, out_specs=out_specs, check_vma=False)
```

```python
import functools
import math

import jax
import jax.numpy as jnp
from jax import lax
from jax.experimental import pallas as pl
from jax.experimental.pallas import tpu as pltpu
from jax.sharding import PartitionSpec as P

MESH = pl.DeviceIdType.MESH
BATCH = 6
WIDTH = 2048
HEAD = 128
STEPS = 24
EPSILON = 1e-06
ROWS = 256
PIECE = 32
HALO = (32, 96, 384)
SPAN = (160, 224, 512)
DILATION = (1, 4, 16)
COPIES = 200
EXCHANGE = 192
F32 = jnp.float32
BF16 = jnp.bfloat16
DELTAS = (0, 1, -1, 2)
LOPSIDED = ('kv0', 'q')
NT = (((1,), (1,)), ((), ()))
TN = (((0,), (0,)), ((), ()))


class Steps:
    pass


class Sender:
    def __init__(self, send_sem, recv_sem):
        self.send_sem, self.recv_sem, self.started = send_sem, recv_sem, []

    def __call__(self, src, dst, device):
        slot = len(self.started)
        copy = pltpu.make_async_remote_copy(
            src_ref=src,
            dst_ref=dst,
            send_sem=self.send_sem.at[slot],
            recv_sem=self.recv_sem.at[slot],
            device_id=device,
            device_id_type=MESH,
        )
        copy.start()
        self.started.append(copy)
        return copy


def plane_tasks(k, lopsided):
    if not lopsided:
        tasks = [
            ("begin", (), [("A+", 0, 0, None, "A+"), ("A-", 0, 0, None, "A-"), ("B+0", 0, 0, None, "B+"), ("B-0", 0, 0, None, "B-")]),
            ("up", ("A+",), [("A++", -1, 0, 0, "A+"), ("B+-1", -1, 0, None, "B+"), ("B--1", -1, 0, None, "B-")]),
            ("down", ("A-",), [("A--", 1, 0, 1, "A-"), ("B+1", 1, 0, None, "B+"), ("B-1", 1, 0, None, "B-")]),
            ("far", ("A++", "A--"), [("B+2", 2, 0, None, "B+"), ("B-2", 2, 0, None, "B-")]),
            ("up0", ("B+0",), [("C0", 0, -1, None, "B+")]),
            ("up3", ("B+-1",), [("C-1", -1, -1, None, "B+")]),
            ("down1", ("B-1",), [("C1", 1, 1, None, "B-")]),
            ("down2", ("B-2",), [("C2", 2, 1, None, "B-")]),
            ("finish", ("B-0", "B--1", "B+1", "B+2", "C0", "C-1", "C1", "C2"), []),
        ]
    else:
        def spread(d):
            return [(f"B-{d}", d, 0, None, "B-"), (f"B+{d}", d, 0, 0, "B+")]

        tasks = [
            ("begin", (), [("A-", 0, 0, None, "A-"), ("A+", 0, 0, 0, "A+"), *spread(0)]),
            ("one", ("A-",), [("A--", 1, 0, None, "A-"), *spread(1)]),
            ("two", ("A--",), [("A---", 2, 0, 1, "A-"), *spread(2)]),
            ("back", ("A+", "A---"), spread(-1)),
        ]
        for d in DELTAS:
            tasks.append((f"next{d % 4}", (f"B-{d}",), [(f"C{d}", d, 1, None, "B-")]))
            tasks.append((f"last{d % 4}", (f"C{d}",), [(f"D{d}", d, 2, 1, "B-")]))
        tasks.append(("finish", tuple(f"{w}{d}" for d in DELTAS for w in ("B+", "D")), []))
    return [
        (f"{k}.{n}", tuple(f"{k}.{w}" for w in needs), [(f"{k}.{key}", *rest) for key, *rest in starts])
        for n, needs, starts in tasks
    ]


def kernel(
    tokens_ref, gain_ref, wq_ref, wk_ref, wv_ref, wo_ref,
    mixed_ref, logs_ref,
    raw, normed, w_kv, w_q, w_out, queries, kv0, kv1, kv2, bias, heads, gathered,
    own_logs, partner_logs, send_sem, recv_sem, local_sem,
):
    s, x = lax.axis_index("sp"), lax.axis_index("tp")
    c, q = s % 2, s // 2
    y, z = q % 4, q // 4
    kv = (kv0, kv1, kv2)
    send = Sender(send_sem, recv_sem)
    tok, out, wide = Steps(), Steps(), Steps()
    kv2_part, kv1_part, kv0_part, q_part, wo_part = (Steps() for _ in range(5))
    parts = {"kv2": kv2_part, "kv1": kv1_part, "kv0": kv0_part, "q": q_part, "wo": wo_part}

    def at(chip, core, column):
        return (chip * 2 + core, column)

    def chip_of(a, b):
        return (1 - c) * (b * 4 + a) + c * (a * 4 + b)

    a, b = (1 - c) * y + c * z, (1 - c) * z + c * y
    xs = {d: (x + d + 4) % 4 for d in (0, 1, -1, 2)}
    partner = at(q, 1 - c, x)
    onward, behind = at((q + 1) % 16, c, x), at((q + 15) % 16, c, x)
    ways = {
        "A+": at(chip_of((a + 1) % 4, b), c, x),
        "A-": at(chip_of((a + 3) % 4, b), c, x),
        "B+": at(chip_of(a, (b + 1) % 4), c, x),
        "B-": at(chip_of(a, (b + 3) % 4), c, x),
        "x+": at(q, c, xs[1]),
        "x-": at(q, c, xs[-1]),
        "p": partner,
        "h": onward,
    }

    sent, seen = {}, set()

    def start(key, src, dst, way):
        sent[key] = send(src, dst, ways[way])

    def arrived(*keys):
        for key in keys:
            if key not in seen:
                seen.add(key)
                sent[key].wait_recv()

    def local(src, dst, slot):
        copy = pltpu.make_async_copy(src, dst, local_sem.at[slot])
        copy.start()
        return copy

    load = local(tokens_ref, raw, 0)
    mine = pl.ds(pl.multiple_of(q * 128 + c * 64, 64), 64)
    own_columns = pl.ds(pl.multiple_of(c * HEAD, HEAD), HEAD)
    other_columns = pl.ds(pl.multiple_of((1 - c) * HEAD, HEAD), HEAD)
    swaps = []
    for g in (2, 1, 0):
        for r, ref in enumerate((wk_ref, wv_ref)):
            swaps.append((f"kv{g}", ref.at[g], w_kv.at[g, mine, pl.ds(r * HEAD, HEAD)]))
    for g in range(3):
        swaps.append(("q", wq_ref.at[g], w_q.at[mine, pl.ds(g * HEAD, HEAD)]))
    kept = {}
    for i, (k, src, dst) in enumerate(swaps):
        kept.setdefault(k, []).append(local(src.at[:, own_columns], dst, 1 + i))
    x_columns = {d: pl.ds(pl.multiple_of(xs[d] * 256, 256), 256) for d in DELTAS}
    kept["wo"] = [local(wo_ref, w_out.at[q, c, :, x_columns[0]], 10)]

    barrier = pltpu.get_barrier_semaphore()
    peers = [partner, onward, behind] + [ways[w] for w in ("A+", "A-", "B+", "B-")]
    for d in (1, -1, 2):
        peers += [at(q, c, xs[d]), at(q, 1 - c, xs[d])]
    for peer in peers:
        pl.semaphore_signal(barrier, inc=1, device_id=peer, device_id_type=MESH)
    pl.semaphore_wait(barrier, len(peers))

    swapped = {"wo": []}
    for i, (k, src, dst) in enumerate(swaps):
        start(f"swap{i}", src.at[:, other_columns], dst, "p")
        swapped.setdefault(k, []).append(f"swap{i}")

    def slab(core, column):
        return pl.ds(pl.multiple_of(core * 128 + column * PIECE, PIECE), PIECE)

    halves = (pl.ds(0, 3), pl.ds(3, 3))

    def pass_on(key, half, d, way):
        ref = normed.at[halves[half], slab(c, xs[d]), :]
        start(key, ref, ref, way)

    def norm():
        load.wait()
        own_slab = slab(c, x)

        def one(i, _):
            wide = raw[i].astype(F32)
            mean = jnp.sum(wide * wide, axis=-1, keepdims=True) * (1.0 / WIDTH)
            scaled = wide * lax.rsqrt(mean + EPSILON)
            normed[i, own_slab, :] = (scaled * gain_ref[...]).astype(BF16)
            return 0

        lax.fori_loop(0, BATCH, one, 0)
        for half in range(2):
            pass_on(f"x+{half}", half, 0, "x+")
            pass_on(f"x-{1 - half}", 1 - half, 0, "x-")
            pass_on(f"p{half}", half, 0, "p")

    def token_step(needs, starts):
        def run():
            arrived(needs)
            for args in starts:
                pass_on(*args)

        return run

    tok.begin = norm
    tok.a = token_step("x+0", [("x++", 0, -1, "x+"), ("m-1.0", 0, -1, "p")])
    tok.b = token_step("x-1", [("x--", 1, 1, "x-"), ("m1.1", 1, 1, "p")])
    tok.c = token_step("x+1", [("m-1.1", 1, -1, "p")])
    tok.d = token_step("x-0", [("m1.0", 0, 1, "p")])
    tok.e = token_step("x++", [("m2.0", 0, 2, "p")])
    tok.f = token_step("x--", [("m2.1", 1, 2, "p")])
    token_needs = {0: ("p0", "p1")}
    token_needs[-1] = ("x+0", "x+1", "m-1.0", "m-1.1")
    token_needs[1] = ("x-0", "x-1", "m1.0", "m1.1")
    token_needs[2] = ("x++", "x--", "m2.0", "m2.1")

    def block(k, da, db, half):
        chip = chip_of((a + da + 4) % 4, (b + db + 4) % 4)
        if k == "wo":
            rows = pl.ds(0, 64) if half is None else pl.ds(32 * half, 32)
            return w_out.at[chip, c, rows, x_columns[0]]
        if half is None:
            rows = pl.ds(pl.multiple_of(chip * 128, 128), 128)
        else:
            rows = pl.ds(pl.multiple_of(chip * 128 + 64 * half, 64), 64)
        return w_q.at[rows, :] if k == "q" else w_kv.at[int(k[2]), rows, :]

    def plane_step(k, name, needs, starts):
        def run():
            if name.endswith("begin"):
                for copy in kept[k]:
                    copy.wait()
                arrived(*swapped[k])
            arrived(*needs)
            for key, da, db, half, way in starts:
                ref = block(k, da, db, half)
                start(key, ref, ref, way)

        return run

    for k in ("kv2", "kv1", "kv0", "q", "wo"):
        for name, needs, starts in plane_tasks(k, k in LOPSIDED):
            setattr(parts[k], name.split(".")[1], plane_step(k, name, needs, starts))

    out_halves = (pl.ds(0, 8), pl.ds(8, 8), pl.ds(0, 16))

    def pass_out(key, half, d, way):
        ref = w_out.at[out_halves[half], c, :, x_columns[d]]
        start(key, ref, ref, way)

    def out_step(needs, starts):
        def run():
            arrived(*needs)
            for args in starts:
                pass_out(*args)

        return run

    out.begin = out_step((), [
        ("o+0", 0, 0, "x+"), ("o-1", 1, 0, "x-"), ("o+1", 1, 0, "x+"), ("o-0", 0, 0, "x-"), ("n0", 2, 0, "p")
    ])
    out.a = out_step(("o+0",), [("o++", 0, -1, "x+")])
    out.b = out_step(("o-1",), [("o--", 1, 1, "x-")])
    out.c = out_step(("o+0", "o+1"), [("n-1", 2, -1, "p")])
    out.d = out_step(("o-0", "o-1"), [("n1", 2, 1, "p")])
    out.e = out_step(("o++", "o--"), [("n2", 2, 2, "p")])

    def rows_of(i, d):
        return normed[:, slab(i, xs[d]), :].reshape(BATCH * PIECE, WIDTH)

    def project_kv(g, d):
        def one(i, _):
            product = jnp.dot(rows_of(i, d), w_kv[g], preferred_element_type=F32).astype(BF16)
            first = pl.multiple_of(HALO[g] + i * 128 + xs[d] * PIECE, PIECE)
            kv[g][:, pl.ds(first, PIECE), :] = product.reshape(BATCH, PIECE, 2 * HEAD)
            return 0

        def run():
            arrived(*token_needs[d])
            lax.fori_loop(0, 2, one, 0)
            if g == 2:
                for core in (1, 0):
                    first = core * 128 + xs[d] * PIECE
                    start(
                        f"w{core}.{d}",
                        kv2.at[:, pl.ds(pl.multiple_of(384 + first, PIECE), PIECE), :],
                        kv2.at[:, pl.ds(pl.multiple_of(128 + first, PIECE), PIECE), :],
                        "h",
                    )

        return run

    def project_q(d):
        def one(i, _):
            product = jnp.dot(rows_of(i, d), w_q[...], preferred_element_type=F32).astype(BF16)
            for g in range(3):
                part = product[:, g * HEAD : (g + 1) * HEAD].reshape(BATCH, PIECE, HEAD)
                queries[g, :, slab(i, xs[d]), :] = part
            return 0

        def run():
            arrived(*token_needs[d])
            lax.fori_loop(0, 2, one, 0)

        return run

    def forward_wide(d):
        def run():
            arrived(f"w1.{d}")
            start(
                f"f.{d}",
                kv2.at[:, pl.ds(pl.multiple_of(256 + xs[d] * PIECE, PIECE), PIECE), :],
                kv2.at[:, slab(0, xs[d]), :],
                "h",
            )

        return run

    for d in DELTAS:
        for g in range(3):
            setattr(parts[f"kv{g}"], f"project{d % 4}", project_kv(g, d))
        setattr(q_part, f"project{d % 4}", project_q(d))
        setattr(wide, f"onward{d % 4}", forward_wide(d))
    kv1_part.halo = lambda: start("mid", kv1.at[:, pl.ds(ROWS, 96), :], kv1.at[:, pl.ds(0, 96), :], "h")
    kv0_part.halo = lambda: start("near", kv0.at[:, pl.ds(ROWS, 32), :], kv0.at[:, pl.ds(0, 32), :], "h")

    def make_masks():
        own_logs[...] = jnp.zeros_like(own_logs)
        for half in range(2):
            row = 0
            for g in (2, 1, 0):
                key = lax.broadcasted_iota(jnp.int32, (SPAN[g], 128), 0)
                lane = lax.broadcasted_iota(jnp.int32, (SPAN[g], 128), 1)
                lag = lane - key + HALO[g]
                position = key + (half * 128 - HALO[g]) + q * ROWS
                met = (lag >= 0) & (lag <= STEPS * DILATION[g]) & (position >= 0)
                if DILATION[g] > 1:
                    met = met & ((lag & (DILATION[g] - 1)) == 0)
                bias[half, row : row + SPAN[g], :] = jnp.where(met, F32(0), F32(-1e30))
                row += SPAN[g]

    scale = 1.0 / math.sqrt(HEAD)
    column_of_mine = pl.ds(pl.multiple_of((2 * x + c) * HEAD, HEAD), HEAD)

    def attend(half):
        def one(i, _):
            parts, row = [], 0
            for g in (2, 1, 0):
                keys = kv[g][i, pl.ds(half * 128, SPAN[g]), pl.ds(0, HEAD)]
                query = queries[g, i, pl.ds(half * 128, 128), :]
                score = lax.dot_general(keys, query, NT, preferred_element_type=F32)
                parts.append(score * scale + bias[half, row : row + SPAN[g], :])
                row += SPAN[g]
            peak = functools.reduce(jnp.maximum, [jnp.max(p, axis=0, keepdims=True) for p in parts])
            total = jnp.zeros((1, 128), F32)
            mixture = jnp.zeros((HEAD, 128), F32)
            for g, part in zip((2, 1, 0), parts):
                lifted = jnp.exp(part - peak)
                total = total + jnp.sum(lifted, axis=0, keepdims=True)
                values = kv[g][i, pl.ds(half * 128, SPAN[g]), pl.ds(HEAD, HEAD)]
                mixture = mixture + lax.dot_general(
                    values, lifted.astype(BF16), TN, preferred_element_type=F32
                )
            own_logs[half, pl.ds(i, 1), :] = peak + jnp.log(total)
            heads[i, pl.ds(half * 128, 128), :] = (mixture / total).T.astype(BF16)
            return 0

        lax.fori_loop(0, BATCH, one, 0, unroll=2)

    exchanged = []

    def exchange(half):
        for i, d in enumerate((2, 1, -1)):
            copy = pltpu.make_async_remote_copy(
                src_ref=heads.at[:, slab(half, xs[d]), :],
                dst_ref=gathered.at[:, :, column_of_mine],
                send_sem=send_sem.at[EXCHANGE + 2 * i + half],
                recv_sem=recv_sem.at[EXCHANGE + 2 * i + c],
                device_id=at(q, half, xs[d]),
                device_id_type=MESH,
            )
            copy.start()
            exchanged.append(copy)

    make_masks()
    order = (
        tok.begin, kv2_part.begin, kv1_part.begin, kv2_part.up, kv2_part.down, kv2_part.up0,
        kv1_part.up, kv1_part.down, kv1_part.up0, kv2_part.far, kv2_part.up3, kv2_part.down1,
        kv1_part.far, kv0_part.begin, wo_part.begin, kv1_part.up3, kv1_part.down1, kv2_part.down2,
        tok.a, tok.b, kv0_part.one, wo_part.up, wo_part.down, kv1_part.down2,
        kv0_part.next0, wo_part.up0, q_part.begin, kv0_part.two, wo_part.far, kv2_part.finish,
        wo_part.up3, kv2_part.project0, kv0_part.next1, wo_part.down1, q_part.one, tok.c,
        tok.d, kv0_part.back, kv1_part.finish, kv1_part.project0, kv0_part.last0, kv2_part.project3,
        wide.onward0, q_part.next0, kv2_part.project1, q_part.two, kv0_part.next2, kv1_part.project1,
        wo_part.down2, kv1_part.project3, kv0_part.last1, q_part.next1, q_part.back, kv0_part.next3,
        wide.onward3, tok.e, tok.f, q_part.last0, q_part.next2, kv0_part.last2,
        wo_part.finish, out.begin, kv2_part.project2, kv1_part.project2, kv1_part.halo, q_part.last1,
        q_part.next3, kv0_part.last3, wide.onward1, q_part.last2, q_part.last3, kv0_part.finish,
        kv0_part.project0, out.a, out.b, kv0_part.project1, kv0_part.project3, q_part.finish,
        kv0_part.project2, kv0_part.halo, wide.onward2, q_part.project0, q_part.project1, q_part.project3,
        out.c, out.d, q_part.project2, out.e,
    )
    for step in order:
        step()

    arrived(*(f"w{core}.{d}" for core in (1, 0) for d in DELTAS), "mid", "near")
    attend(1)
    exchange(1)
    arrived(*(f"f.{d}" for d in DELTAS))
    attend(0)
    exchange(0)
    start("logs", own_logs.at[1 - c], partner_logs, "p")
    start("heads", heads.at[:, slab(1 - c, x), :], gathered.at[:, :, column_of_mine], "p")
    stay = local(heads.at[:, slab(c, x), :], gathered.at[:, :, column_of_mine], 11)
    arrived("n0", "n1", "n-1", "n2", "logs")
    mine_logs, their_logs = own_logs[c], partner_logs[...]
    logs_ref[:, 0, :] = jnp.where(c == 0, mine_logs, their_logs)[:BATCH]
    logs_ref[:, 1, :] = jnp.where(c == 0, their_logs, mine_logs)[:BATCH]
    stay.wait()
    arrived("heads")
    for slot in range(6):
        pltpu.make_async_remote_copy(
            src_ref=heads.at[:, pl.ds(0, PIECE), :],
            dst_ref=gathered.at[:, :, column_of_mine],
            send_sem=send_sem.at[EXCHANGE + slot],
            recv_sem=recv_sem.at[EXCHANGE + slot],
            device_id=partner,
            device_id_type=MESH,
        ).wait_recv()

    combined = gathered[...].reshape(BATCH * PIECE, 8 * HEAD)

    def out_tile(i, _):
        tile = w_out[pl.ds(i * 4, 4)].reshape(512, 8 * HEAD)
        product = lax.dot_general(combined, tile, NT, preferred_element_type=F32)
        columns = pl.ds(pl.multiple_of(i * 512, 512), 512)
        mixed_ref[:, :, columns] = product.astype(BF16).reshape(BATCH, PIECE, 512)
        return 0

    lax.fori_loop(0, 4, out_tile, 0)
    for copy in send.started + exchanged:
        copy.wait_send()


def layer(tokens, norm_gain, w_query, w_key, w_value, w_out):
    any_space = pl.BlockSpec(memory_space=pl.ANY)
    vmem = pl.BlockSpec(memory_space=pltpu.VMEM)
    mixed, logs = pl.pallas_call(
        kernel,
        out_shape=(
            jax.ShapeDtypeStruct((BATCH, PIECE, WIDTH), BF16),
            jax.ShapeDtypeStruct((BATCH, 2, 128), F32),
        ),
        in_specs=[any_space, vmem, any_space, any_space, any_space, any_space],
        out_specs=(vmem, vmem),
        scratch_shapes=[
            pltpu.VMEM((BATCH, PIECE, WIDTH), BF16),
            pltpu.VMEM((BATCH, ROWS, WIDTH), BF16),
            pltpu.VMEM((3, WIDTH, 2 * HEAD), BF16),
            pltpu.VMEM((WIDTH, 3 * HEAD), BF16),
            pltpu.VMEM((16, 2, 64, 8 * HEAD), BF16),
            pltpu.VMEM((3, BATCH, ROWS, HEAD), BF16),
            pltpu.VMEM((BATCH, HALO[0] + ROWS, 2 * HEAD), BF16),
            pltpu.VMEM((BATCH, HALO[1] + ROWS, 2 * HEAD), BF16),
            pltpu.VMEM((BATCH, HALO[2] + ROWS, 2 * HEAD), BF16),
            pltpu.VMEM((2, sum(SPAN), 128), F32),
            pltpu.VMEM((BATCH, ROWS, HEAD), BF16),
            pltpu.VMEM((BATCH, PIECE, 8 * HEAD), BF16),
            pltpu.VMEM((2, 8, 128), F32),
            pltpu.VMEM((8, 128), F32),
            pltpu.SemaphoreType.DMA((COPIES,)),
            pltpu.SemaphoreType.DMA((COPIES,)),
            pltpu.SemaphoreType.DMA((12,)),
        ],
        compiler_params=pltpu.CompilerParams(
            collective_id=0, has_side_effects=True, vmem_limit_bytes=56 * 1024 * 1024
        ),
    )(
        jnp.transpose(tokens, (1, 0, 2)),
        norm_gain.reshape(1, WIDTH),
        w_query,
        w_key,
        w_value,
        jnp.transpose(w_out),
    )
    return jnp.transpose(mixed, (1, 0, 2)), jnp.transpose(logs, (2, 0, 1))


def solution(mesh):
    in_specs = (
        P(("sp", "tp"), None, None),
        P(),
        P(None, "sp", "tp"),
        P(None, "sp", "tp"),
        P(None, "sp", "tp"),
        P("tp", "sp"),
    )
    out_specs = (P(("sp", "tp"), None, None), P("sp", None, "tp"))
    return jax.shard_map(layer, mesh=mesh, in_specs=in_specs, out_specs=out_specs, check_vma=False)
```

```python
import functools
import math

import jax
import jax.numpy as jnp
from jax import lax
from jax.experimental import pallas as pl
from jax.experimental.pallas import tpu as pltpu
from jax.sharding import PartitionSpec as P

MESH = pl.DeviceIdType.MESH
BATCH = 6
WIDTH = 2048
HEAD = 128
STEPS = 24
EPSILON = 1e-06
ROWS = 256
PIECE = 32
HALO = (32, 96, 384)
SPAN = (160, 224, 512)
DILATION = (1, 4, 16)
COPIES = 200
EXCHANGE = 192
F32 = jnp.float32
BF16 = jnp.bfloat16
DELTAS = (0, 1, -1, 2)
LEAN = {"kv2": 0, "kv1": 0, "kv0": 2, "q": 2, "wo": 2}
NT = (((1,), (1,)), ((), ()))
TN = (((0,), (0,)), ((), ()))


class Steps:
    pass


class Sender:
    def __init__(self, send_sem, recv_sem):
        self.send_sem, self.recv_sem, self.started, self.count = send_sem, recv_sem, [], 0

    def __call__(self, src, dst, device):
        copy = self.prepare(src, dst, device)
        copy.start()
        self.started.append(copy)
        return copy

    def prepare(self, src, dst, device):
        slot = self.count
        self.count += 1
        return pltpu.make_async_remote_copy(
            src_ref=src,
            dst_ref=dst,
            send_sem=self.send_sem.at[slot],
            recv_sem=self.recv_sem.at[slot],
            device_id=device,
            device_id_type=MESH,
        )


def plane_tasks(k, lean):
    if lean == 0:
        tasks = [
            ("begin", (), [("A+", 0, 0, None, "A+"), ("A-", 0, 0, None, "A-"), ("B+0", 0, 0, None, "B+"), ("B-0", 0, 0, None, "B-")]),
            ("up", ("A+",), [("A++", -1, 0, 0, "A+"), ("B+-1", -1, 0, None, "B+"), ("B--1", -1, 0, None, "B-")]),
            ("down", ("A-",), [("A--", 1, 0, 1, "A-"), ("B+1", 1, 0, None, "B+"), ("B-1", 1, 0, None, "B-")]),
            ("far", ("A++", "A--"), [("B+2", 2, 0, None, "B+"), ("B-2", 2, 0, None, "B-")]),
            ("up0", ("B+0",), [("C0", 0, -1, None, "B+")]),
            ("up3", ("B+-1",), [("C-1", -1, -1, None, "B+")]),
            ("down1", ("B-1",), [("C1", 1, 1, None, "B-")]),
            ("down2", ("B-2",), [("C2", 2, 1, None, "B-")]),
            ("finish", ("B-0", "B--1", "B+1", "B+2", "C0", "C-1", "C1", "C2"), []),
        ]
    else:
        last = 1 if lean == 1 else None

        def spread(d):
            up = [(f"B+{d}", d, 0, 0, "B+")] if lean == 1 else []
            return [(f"B-{d}", d, 0, None, "B-"), *up]

        first_up = [("A+", 0, 0, 0, "A+")] if lean == 1 else []
        tasks = [
            ("begin", (), [("A-", 0, 0, None, "A-"), *first_up, *spread(0)]),
            ("one", ("A-",), [("A--", 1, 0, None, "A-"), *spread(1)]),
            ("two", ("A--",), [("A---", 2, 0, last, "A-"), *spread(2)]),
            ("back", ("A---", "A+")[: 3 - lean], spread(-1)),
        ]
        for d in DELTAS:
            tasks.append((f"next{d % 4}", (f"B-{d}",), [(f"C{d}", d, 1, None, "B-")]))
            tasks.append((f"last{d % 4}", (f"C{d}",), [(f"D{d}", d, 2, last, "B-")]))
        ends = ("D", "B+")[: 3 - lean]
        tasks.append(("finish", tuple(f"{w}{d}" for d in DELTAS for w in ends), []))
    return [
        (f"{k}.{n}", tuple(f"{k}.{w}" for w in needs), [(f"{k}.{key}", *rest) for key, *rest in starts])
        for n, needs, starts in tasks
    ]


def kernel(
    tokens_ref, gain_ref, wq_ref, wk_ref, wv_ref, wo_ref,
    mixed_ref, logs_ref,
    raw, normed, w_kv, w_q, w_out, queries, kv0, kv1, kv2, bias, heads, gathered,
    own_logs, partner_logs, send_sem, recv_sem, local_sem,
):
    s, x = lax.axis_index("sp"), lax.axis_index("tp")
    c, q = s % 2, s // 2
    y, z = q % 4, q // 4
    kv = (kv0, kv1, kv2)
    send = Sender(send_sem, recv_sem)
    tok, out, wide = Steps(), Steps(), Steps()
    kv2_part, kv1_part, kv0_part, q_part, wo_part = (Steps() for _ in range(5))
    parts = {"kv2": kv2_part, "kv1": kv1_part, "kv0": kv0_part, "q": q_part, "wo": wo_part}

    def at(chip, core, column):
        return (chip * 2 + core, column)

    def chip_of(a, b):
        return (1 - c) * (b * 4 + a) + c * (a * 4 + b)

    a, b = (1 - c) * y + c * z, (1 - c) * z + c * y
    xs = {d: (x + d + 4) % 4 for d in (0, 1, -1, 2)}
    partner = at(q, 1 - c, x)
    onward, behind = at((q + 1) % 16, c, x), at((q + 15) % 16, c, x)
    ways = {
        "A+": at(chip_of((a + 1) % 4, b), c, x),
        "A-": at(chip_of((a + 3) % 4, b), c, x),
        "B+": at(chip_of(a, (b + 1) % 4), c, x),
        "B-": at(chip_of(a, (b + 3) % 4), c, x),
        "x+": at(q, c, xs[1]),
        "x-": at(q, c, xs[-1]),
        "p": partner,
        "h": onward,
    }

    sent, seen = {}, set()

    def start(key, src, dst, way):
        sent[key] = send(src, dst, ways[way])

    def arrived(*keys):
        for key in keys:
            if key not in seen:
                seen.add(key)
                sent[key].wait_recv()

    def local(src, dst, slot):
        copy = pltpu.make_async_copy(src, dst, local_sem.at[slot])
        copy.start()
        return copy

    load = local(tokens_ref, raw, 0)
    mine = pl.ds(pl.multiple_of(q * 128 + c * 64, 64), 64)
    own_columns = pl.ds(pl.multiple_of(c * HEAD, HEAD), HEAD)
    other_columns = pl.ds(pl.multiple_of((1 - c) * HEAD, HEAD), HEAD)
    swaps = []
    for g in (2, 1, 0):
        for r, ref in enumerate((wk_ref, wv_ref)):
            swaps.append((f"kv{g}", ref.at[g], w_kv.at[g, mine, pl.ds(r * HEAD, HEAD)]))
    for g in range(3):
        swaps.append(("q", wq_ref.at[g], w_q.at[mine, pl.ds(g * HEAD, HEAD)]))
    kept = {}
    for i, (k, src, dst) in enumerate(swaps):
        kept.setdefault(k, []).append(local(src.at[:, own_columns], dst, 1 + i))
    x_columns = {d: pl.ds(pl.multiple_of(xs[d] * 256, 256), 256) for d in DELTAS}
    kept["wo"] = [local(wo_ref, w_out.at[q, c, :, x_columns[0]], 10)]

    barrier = pltpu.get_barrier_semaphore()
    peers = [partner, onward, behind] + [ways[w] for w in ("A+", "A-", "B+", "B-")]
    for d in (1, -1, 2):
        peers += [at(q, c, xs[d]), at(q, 1 - c, xs[d])]
    for peer in peers:
        pl.semaphore_signal(barrier, inc=1, device_id=peer, device_id_type=MESH)
    pl.semaphore_wait(barrier, len(peers))

    swapped = {"wo": []}
    for i, (k, src, dst) in enumerate(swaps):
        start(f"swap{i}", src.at[:, other_columns], dst, "p")
        swapped.setdefault(k, []).append(f"swap{i}")

    def slab(core, column):
        return pl.ds(pl.multiple_of(core * 128 + column * PIECE, PIECE), PIECE)

    halves = (pl.ds(0, 3), pl.ds(3, 3))

    def pass_on(key, half, d, way):
        ref = normed.at[halves[half], slab(c, xs[d]), :]
        start(key, ref, ref, way)

    def norm():
        load.wait()
        own_slab = slab(c, x)

        def one(i, _):
            wide = raw[i].astype(F32)
            mean = jnp.sum(wide * wide, axis=-1, keepdims=True) * (1.0 / WIDTH)
            scaled = wide * lax.rsqrt(mean + EPSILON)
            normed[i, own_slab, :] = (scaled * gain_ref[...]).astype(BF16)
            return 0

        lax.fori_loop(0, BATCH, one, 0)
        for half in range(2):
            pass_on(f"x+{half}", half, 0, "x+")
            pass_on(f"x-{1 - half}", 1 - half, 0, "x-")
            pass_on(f"p{half}", half, 0, "p")

    def token_step(needs, starts):
        def run():
            arrived(needs)
            for args in starts:
                pass_on(*args)

        return run

    tok.begin = norm
    tok.a = token_step("x+0", [("x++", 0, -1, "x+"), ("m-1.0", 0, -1, "p")])
    tok.b = token_step("x-1", [("x--", 1, 1, "x-"), ("m1.1", 1, 1, "p")])
    tok.c = token_step("x+1", [("m-1.1", 1, -1, "p")])
    tok.d = token_step("x-0", [("m1.0", 0, 1, "p")])
    tok.e = token_step("x++", [("m2.0", 0, 2, "p")])
    tok.f = token_step("x--", [("m2.1", 1, 2, "p")])

    def token_needs(d, half):
        if d == 0:
            return (f"p{half}",)
        if d == 2:
            return (("x++", "x--")[half], f"m2.{half}")
        return (("x-" if d == 1 else "x+") + str(half), f"m{d}.{half}")

    def block(k, da, db, half):
        chip = chip_of((a + da + 4) % 4, (b + db + 4) % 4)
        if k == "wo":
            rows = pl.ds(0, 64) if half is None else pl.ds(32 * half, 32)
            return w_out.at[chip, c, rows, x_columns[0]]
        if half is None:
            rows = pl.ds(pl.multiple_of(chip * 128, 128), 128)
        else:
            rows = pl.ds(pl.multiple_of(chip * 128 + 64 * half, 64), 64)
        return w_q.at[rows, :] if k == "q" else w_kv.at[int(k[2]), rows, :]

    def plane_step(k, name, needs, starts):
        def run():
            if name.endswith("begin"):
                for copy in kept[k]:
                    copy.wait()
                arrived(*swapped[k])
            arrived(*needs)
            for key, da, db, half, way in starts:
                ref = block(k, da, db, half)
                start(key, ref, ref, way)

        return run

    for k in ("kv2", "kv1", "kv0", "q", "wo"):
        for name, needs, starts in plane_tasks(k, LEAN[k]):
            setattr(parts[k], name.split(".")[1], plane_step(k, name, needs, starts))

    out_halves = (pl.ds(0, 8), pl.ds(8, 8), pl.ds(0, 16))

    def pass_out(key, half, d, way):
        ref = w_out.at[out_halves[half], c, :, x_columns[d]]
        start(key, ref, ref, way)

    def out_step(needs, starts):
        def run():
            arrived(*needs)
            for args in starts:
                pass_out(*args)

        return run

    out.begin = out_step((), [
        ("o+0", 0, 0, "x+"), ("o-1", 1, 0, "x-"), ("o+1", 1, 0, "x+"), ("o-0", 0, 0, "x-"), ("n0", 2, 0, "p")
    ])
    out.a = out_step(("o+0",), [("o++", 0, -1, "x+")])
    out.b = out_step(("o-1",), [("o--", 1, 1, "x-")])
    out.c = out_step(("o+0", "o+1"), [("n-1", 2, -1, "p")])
    out.d = out_step(("o-0", "o-1"), [("n1", 2, 1, "p")])
    out.e = out_step(("o++", "o--"), [("n2", 2, 2, "p")])

    def rows_of(d, part=pl.ds(0, BATCH)):
        pieces = [normed[part, slab(core, xs[d]), :] for core in range(2)]
        return jnp.concatenate([p.reshape(-1, WIDTH) for p in pieces], axis=0)

    def need_tokens(d):
        for half in range(2):
            arrived(*token_needs(d, half))

    def keep_kv(g, d, product, part=pl.ds(0, BATCH)):
        product = product.astype(BF16).reshape(2, -1, PIECE, 2 * HEAD)
        for core in range(2):
            first = pl.multiple_of(HALO[g] + core * 128 + xs[d] * PIECE, PIECE)
            kv[g][part, pl.ds(first, PIECE), :] = product[core]

    def at_wide(half, base, core, d):
        first = pl.multiple_of(base + core * 128 + xs[d] * PIECE, PIECE)
        return kv2.at[halves[half], pl.ds(first, PIECE), :]

    def project_wide(d, half):
        def run():
            arrived(*token_needs(d, half))
            part = halves[half]
            keep_kv(2, d, jnp.dot(rows_of(d, part), w_kv[2], preferred_element_type=F32), part)
            for core in (1, 0):
                start(f"w{core}{d}{half}", at_wide(half, 384, core, d), at_wide(half, 128, core, d), "h")

        return run

    def forward_wide(d, half):
        def run():
            arrived(f"w1{d}{half}")
            start(f"f{d}{half}", at_wide(half, 256, 0, d), at_wide(half, 0, 0, d), "h")

        return run

    near = send.prepare(kv0.at[:, pl.ds(ROWS, 32), :], kv0.at[:, pl.ds(0, 32), :], onward)
    middle = {}
    for d in DELTAS:
        to = pl.multiple_of(jnp.maximum(xs[d] - 1, 0) * PIECE, PIECE)
        own = pl.multiple_of(96 + 128 + jnp.maximum(xs[d], 1) * PIECE, PIECE)
        middle[d] = send.prepare(kv1.at[:, pl.ds(own, PIECE), :], kv1.at[:, pl.ds(to, PIECE), :], onward)

    def project_kv(g, d):
        def run():
            need_tokens(d)
            keep_kv(g, d, jnp.dot(rows_of(d), w_kv[g], preferred_element_type=F32))
            if g == 1:
                pl.when(xs[d] > 0)(middle[d].start)
            else:
                pl.when(xs[d] == 3)(near.start)

        return run

    def project_q(d):
        def run():
            need_tokens(d)
            product = jnp.dot(rows_of(d), w_q[...], preferred_element_type=F32)
            product = product.astype(BF16).reshape(2, BATCH, PIECE, 3 * HEAD)
            for core in range(2):
                for g in range(3):
                    queries[g, :, slab(core, xs[d]), :] = product[core, :, :, g * HEAD : (g + 1) * HEAD]

        return run

    for d in DELTAS:
        for half in range(2):
            setattr(kv2_part, f"project{d % 4}{half}", project_wide(d, half))
            setattr(wide, f"onward{d % 4}{half}", forward_wide(d, half))
        setattr(kv1_part, f"project{d % 4}", project_kv(1, d))
        setattr(kv0_part, f"project{d % 4}", project_kv(0, d))
        setattr(q_part, f"project{d % 4}", project_q(d))

    def make_masks():
        own_logs[...] = jnp.zeros_like(own_logs)
        for half in range(2):
            row = 0
            for g in (2, 1, 0):
                key = lax.broadcasted_iota(jnp.int32, (SPAN[g], 128), 0)
                lane = lax.broadcasted_iota(jnp.int32, (SPAN[g], 128), 1)
                lag = lane - key + HALO[g]
                position = key + (half * 128 - HALO[g]) + q * ROWS
                met = (lag >= 0) & (lag <= STEPS * DILATION[g]) & (position >= 0)
                if DILATION[g] > 1:
                    met = met & ((lag & (DILATION[g] - 1)) == 0)
                bias[half, row : row + SPAN[g], :] = jnp.where(met, F32(0), F32(-1e30))
                row += SPAN[g]

    scale = 1.0 / math.sqrt(HEAD)
    column_of_mine = pl.ds(pl.multiple_of((2 * x + c) * HEAD, HEAD), HEAD)

    def attend(half):
        def one(i, _):
            parts, row = [], 0
            for g in (2, 1, 0):
                keys = kv[g][i, pl.ds(half * 128, SPAN[g]), pl.ds(0, HEAD)]
                query = queries[g, i, pl.ds(half * 128, 128), :]
                score = lax.dot_general(keys, query, NT, preferred_element_type=F32)
                parts.append(score * scale + bias[half, row : row + SPAN[g], :])
                row += SPAN[g]
            peak = functools.reduce(jnp.maximum, [jnp.max(p, axis=0, keepdims=True) for p in parts])
            total = jnp.zeros((1, 128), F32)
            mixture = jnp.zeros((HEAD, 128), F32)
            for g, part in zip((2, 1, 0), parts):
                lifted = jnp.exp(part - peak)
                total = total + jnp.sum(lifted, axis=0, keepdims=True)
                values = kv[g][i, pl.ds(half * 128, SPAN[g]), pl.ds(HEAD, HEAD)]
                mixture = mixture + lax.dot_general(
                    values, lifted.astype(BF16), TN, preferred_element_type=F32
                )
            own_logs[half, pl.ds(i, 1), :] = peak + jnp.log(total)
            heads[i, pl.ds(half * 128, 128), :] = (mixture / total).T.astype(BF16)
            return 0

        lax.fori_loop(0, BATCH, one, 0, unroll=2)

    exchanged = []

    def exchange(half):
        for i, d in enumerate((2, 1, -1)):
            copy = pltpu.make_async_remote_copy(
                src_ref=heads.at[:, slab(half, xs[d]), :],
                dst_ref=gathered.at[:, :, column_of_mine],
                send_sem=send_sem.at[EXCHANGE + 2 * i + half],
                recv_sem=recv_sem.at[EXCHANGE + 2 * i + c],
                device_id=at(q, half, xs[d]),
                device_id_type=MESH,
            )
            copy.start()
            exchanged.append(copy)

    make_masks()
    order = (
        kv2_part.begin, tok.begin, kv1_part.begin, kv2_part.up, kv2_part.down, kv2_part.up0,
        kv1_part.up, kv1_part.down, kv1_part.up0, kv2_part.far, kv2_part.up3, kv2_part.down1,
        kv1_part.far, wo_part.begin, kv1_part.up3, kv1_part.down1, kv2_part.down2, wo_part.one,
        tok.a, tok.b, kv1_part.down2, wo_part.next0, kv0_part.begin, wo_part.two,
        kv2_part.finish, kv2_part.project00, wo_part.next1, kv2_part.project01, kv2_part.project30, kv2_part.project11,
        kv0_part.one, kv1_part.finish, kv1_part.project0, wo_part.back, wo_part.last0, kv0_part.next0,
        q_part.begin, wide.onward00, wo_part.next2, wo_part.last1, kv0_part.two, kv0_part.next1,
        wide.onward01, wo_part.next3, tok.c, tok.d, q_part.one, wide.onward30,
        kv2_part.project31, kv0_part.last0, kv1_part.project3, kv0_part.back, kv2_part.project10, kv1_part.project1,
        q_part.next0, wide.onward11, wo_part.last2, q_part.two, kv0_part.next2, kv0_part.last1,
        wo_part.last3, tok.e, tok.f, q_part.next1, q_part.back, kv2_part.project20,
        kv0_part.next3, wide.onward31, kv2_part.project21, q_part.last0, kv1_part.project2, q_part.next2,
        kv0_part.last2, wide.onward10, wo_part.finish, out.begin, q_part.last1, q_part.next3,
        kv0_part.last3, wide.onward20, q_part.last2, wide.onward21, out.a, out.b,
        q_part.last3, kv0_part.finish, kv0_part.project0, kv0_part.project1, kv0_part.project3, kv0_part.project2,
        q_part.finish, q_part.project0, q_part.project1, out.c, out.d, q_part.project3,
        q_part.project2, out.e,
    )
    for step in order:
        step()

    arrived(*(f"w{core}{d}{half}" for core in (1, 0) for d in DELTAS for half in range(2)))
    for d in DELTAS:
        pl.when(xs[d] > 0)(middle[d].wait_recv)
    near.wait_recv()
    attend(1)
    exchange(1)
    arrived(*(f"f{d}{half}" for d in DELTAS for half in range(2)))
    attend(0)
    exchange(0)
    start("logs", own_logs.at[1 - c], partner_logs, "p")
    start("heads", heads.at[:, slab(1 - c, x), :], gathered.at[:, :, column_of_mine], "p")
    stay = local(heads.at[:, slab(c, x), :], gathered.at[:, :, column_of_mine], 11)
    arrived("n0", "n1", "n-1", "n2", "logs")
    mine_logs, their_logs = own_logs[c], partner_logs[...]
    logs_ref[:, 0, :] = jnp.where(c == 0, mine_logs, their_logs)[:BATCH]
    logs_ref[:, 1, :] = jnp.where(c == 0, their_logs, mine_logs)[:BATCH]
    stay.wait()
    arrived("heads")
    for slot in range(6):
        pltpu.make_async_remote_copy(
            src_ref=heads.at[:, pl.ds(0, PIECE), :],
            dst_ref=gathered.at[:, :, column_of_mine],
            send_sem=send_sem.at[EXCHANGE + slot],
            recv_sem=recv_sem.at[EXCHANGE + slot],
            device_id=partner,
            device_id_type=MESH,
        ).wait_recv()

    combined = gathered[...].reshape(BATCH * PIECE, 8 * HEAD)

    def out_tile(i, _):
        tile = w_out[pl.ds(i * 4, 4)].reshape(512, 8 * HEAD)
        product = lax.dot_general(combined, tile, NT, preferred_element_type=F32)
        columns = pl.ds(pl.multiple_of(i * 512, 512), 512)
        mixed_ref[:, :, columns] = product.astype(BF16).reshape(BATCH, PIECE, 512)
        return 0

    lax.fori_loop(0, 4, out_tile, 0)
    for copy in send.started + exchanged + [near]:
        copy.wait_send()
    for d in DELTAS:
        pl.when(xs[d] > 0)(middle[d].wait_send)


def layer(tokens, norm_gain, w_query, w_key, w_value, w_out):
    any_space = pl.BlockSpec(memory_space=pl.ANY)
    vmem = pl.BlockSpec(memory_space=pltpu.VMEM)
    mixed, logs = pl.pallas_call(
        kernel,
        out_shape=(
            jax.ShapeDtypeStruct((BATCH, PIECE, WIDTH), BF16),
            jax.ShapeDtypeStruct((BATCH, 2, 128), F32),
        ),
        in_specs=[any_space, vmem, any_space, any_space, any_space, any_space],
        out_specs=(vmem, vmem),
        scratch_shapes=[
            pltpu.VMEM((BATCH, PIECE, WIDTH), BF16),
            pltpu.VMEM((BATCH, ROWS, WIDTH), BF16),
            pltpu.VMEM((3, WIDTH, 2 * HEAD), BF16),
            pltpu.VMEM((WIDTH, 3 * HEAD), BF16),
            pltpu.VMEM((16, 2, 64, 8 * HEAD), BF16),
            pltpu.VMEM((3, BATCH, ROWS, HEAD), BF16),
            pltpu.VMEM((BATCH, HALO[0] + ROWS, 2 * HEAD), BF16),
            pltpu.VMEM((BATCH, HALO[1] + ROWS, 2 * HEAD), BF16),
            pltpu.VMEM((BATCH, HALO[2] + ROWS, 2 * HEAD), BF16),
            pltpu.VMEM((2, sum(SPAN), 128), F32),
            pltpu.VMEM((BATCH, ROWS, HEAD), BF16),
            pltpu.VMEM((BATCH, PIECE, 8 * HEAD), BF16),
            pltpu.VMEM((2, 8, 128), F32),
            pltpu.VMEM((8, 128), F32),
            pltpu.SemaphoreType.DMA((COPIES,)),
            pltpu.SemaphoreType.DMA((COPIES,)),
            pltpu.SemaphoreType.DMA((12,)),
        ],
        compiler_params=pltpu.CompilerParams(
            collective_id=0, has_side_effects=True, vmem_limit_bytes=56 * 1024 * 1024
        ),
    )(
        jnp.transpose(tokens, (1, 0, 2)),
        norm_gain.reshape(1, WIDTH),
        w_query,
        w_key,
        w_value,
        jnp.transpose(w_out),
    )
    return jnp.transpose(mixed, (1, 0, 2)), jnp.transpose(logs, (2, 0, 1))


def solution(mesh):
    in_specs = (
        P(("sp", "tp"), None, None),
        P(),
        P(None, "sp", "tp"),
        P(None, "sp", "tp"),
        P(None, "sp", "tp"),
        P("tp", "sp"),
    )
    out_specs = (P(("sp", "tp"), None, None), P("sp", None, "tp"))
    return jax.shard_map(layer, mesh=mesh, in_specs=in_specs, out_specs=out_specs, check_vma=False)
```

```python
import functools
import math

import jax
import jax.numpy as jnp
from jax import lax
from jax.experimental import pallas as pl
from jax.experimental.pallas import tpu as pltpu
from jax.sharding import PartitionSpec as P

MESH = pl.DeviceIdType.MESH
BATCH = 6
WIDTH = 2048
HEAD = 128
STEPS = 24
EPSILON = 1e-06
ROWS = 256
PIECE = 32
HALO = (32, 96, 384)
SPAN = (160, 224, 512)
DILATION = (1, 4, 16)
COPIES = 216
EXCHANGE = 200
F32 = jnp.float32
BF16 = jnp.bfloat16
DELTAS = (0, 1, -1, 2)
LEAN = {"kv2": 0, "kv1": 0, "kv0": 2, "q": 2, "wo": 0}
NT = (((1,), (1,)), ((), ()))
TN = (((0,), (0,)), ((), ()))


class Steps:
    pass


class Sender:
    def __init__(self, send_sem, recv_sem):
        self.send_sem, self.recv_sem, self.started, self.count = send_sem, recv_sem, [], 0

    def __call__(self, src, dst, device):
        copy = self.prepare(src, dst, device)
        copy.start()
        self.started.append(copy)
        return copy

    def prepare(self, src, dst, device):
        slot = self.count
        self.count += 1
        return pltpu.make_async_remote_copy(
            src_ref=src,
            dst_ref=dst,
            send_sem=self.send_sem.at[slot],
            recv_sem=self.recv_sem.at[slot],
            device_id=device,
            device_id_type=MESH,
        )


def plane_tasks(k, lean):
    if lean == 0:
        tasks = [
            ("begin", (), [("A+", 0, 0, None, "A+"), ("A-", 0, 0, None, "A-"), ("B+0", 0, 0, None, "B+"), ("B-0", 0, 0, None, "B-")]),
            ("up", ("A+",), [("A++", -1, 0, 0, "A+"), ("B+-1", -1, 0, None, "B+"), ("B--1", -1, 0, None, "B-")]),
            ("down", ("A-",), [("A--", 1, 0, 1, "A-"), ("B+1", 1, 0, None, "B+"), ("B-1", 1, 0, None, "B-")]),
            ("far", ("A++", "A--"), [("B+2", 2, 0, None, "B+"), ("B-2", 2, 0, None, "B-")]),
            ("up0", ("B+0",), [("C0", 0, -1, None, "B+")]),
            ("up3", ("B+-1",), [("C-1", -1, -1, None, "B+")]),
            ("down1", ("B-1",), [("C1", 1, 1, None, "B-")]),
            ("down2", ("B-2",), [("C2", 2, 1, None, "B-")]),
            ("finish", ("B-0", "B--1", "B+1", "B+2", "C0", "C-1", "C1", "C2"), []),
        ]
    else:
        last = 1 if lean == 1 else None

        def spread(d):
            up = [(f"B+{d}", d, 0, 0, "B+")] if lean == 1 else []
            return [(f"B-{d}", d, 0, None, "B-"), *up]

        first_up = [("A+", 0, 0, 0, "A+")] if lean == 1 else []
        tasks = [
            ("begin", (), [("A-", 0, 0, None, "A-"), *first_up, *spread(0)]),
            ("one", ("A-",), [("A--", 1, 0, None, "A-"), *spread(1)]),
            ("two", ("A--",), [("A---", 2, 0, last, "A-"), *spread(2)]),
            ("back", ("A---", "A+")[: 3 - lean], spread(-1)),
        ]
        for d in DELTAS:
            tasks.append((f"next{d % 4}", (f"B-{d}",), [(f"C{d}", d, 1, None, "B-")]))
            tasks.append((f"last{d % 4}", (f"C{d}",), [(f"D{d}", d, 2, last, "B-")]))
        ends = ("D", "B+")[: 3 - lean]
        tasks.append(("finish", tuple(f"{w}{d}" for d in DELTAS for w in ends), []))
    return [
        (f"{k}.{n}", tuple(f"{k}.{w}" for w in needs), [(f"{k}.{key}", *rest) for key, *rest in starts])
        for n, needs, starts in tasks
    ]


def kernel(
    tokens_ref, gain_ref, wq_ref, wk_ref, wv_ref, wo_ref,
    mixed_ref, logs_ref,
    raw, normed, w_kv, w_q, w_out, queries, kv0, kv1, kv2, bias, heads, gathered,
    own_logs, partner_logs, send_sem, recv_sem, local_sem,
):
    s, x = lax.axis_index("sp"), lax.axis_index("tp")
    c, q = s % 2, s // 2
    y, z = q % 4, q // 4
    kv = (kv0, kv1, kv2)
    send = Sender(send_sem, recv_sem)
    tok, out, wide = Steps(), Steps(), Steps()
    kv2_part, kv1_part, kv0_part, q_part, wo_part = (Steps() for _ in range(5))
    parts = {"kv2": kv2_part, "kv1": kv1_part, "kv0": kv0_part, "q": q_part, "wo": wo_part}

    def at(chip, core, column):
        return (chip * 2 + core, column)

    def chip_of(a, b):
        return (1 - c) * (b * 4 + a) + c * (a * 4 + b)

    a, b = (1 - c) * y + c * z, (1 - c) * z + c * y
    xs = {d: (x + d + 4) % 4 for d in (0, 1, -1, 2)}
    partner = at(q, 1 - c, x)
    onward, behind = at((q + 1) % 16, c, x), at((q + 15) % 16, c, x)
    ways = {
        "A+": at(chip_of((a + 1) % 4, b), c, x),
        "A-": at(chip_of((a + 3) % 4, b), c, x),
        "B+": at(chip_of(a, (b + 1) % 4), c, x),
        "B-": at(chip_of(a, (b + 3) % 4), c, x),
        "x+": at(q, c, xs[1]),
        "x-": at(q, c, xs[-1]),
        "p": partner,
        "h": onward,
    }

    sent, seen = {}, set()

    def start(key, src, dst, way):
        sent[key] = send(src, dst, ways[way])

    def arrived(*keys):
        for key in keys:
            if key not in seen:
                seen.add(key)
                sent[key].wait_recv()

    def local(src, dst, slot):
        copy = pltpu.make_async_copy(src, dst, local_sem.at[slot])
        copy.start()
        return copy

    load = local(tokens_ref, raw, 0)
    mine = pl.ds(pl.multiple_of(q * 128 + c * 64, 64), 64)
    own_columns = pl.ds(pl.multiple_of(c * HEAD, HEAD), HEAD)
    other_columns = pl.ds(pl.multiple_of((1 - c) * HEAD, HEAD), HEAD)
    swaps = []
    for g in (2, 1, 0):
        for r, ref in enumerate((wk_ref, wv_ref)):
            swaps.append((f"kv{g}", ref.at[g], w_kv.at[g, mine, pl.ds(r * HEAD, HEAD)]))
    for g in range(3):
        swaps.append(("q", wq_ref.at[g], w_q.at[mine, pl.ds(g * HEAD, HEAD)]))
    kept = {}
    for i, (k, src, dst) in enumerate(swaps):
        kept.setdefault(k, []).append(local(src.at[:, own_columns], dst, 1 + i))
    x_columns = {d: pl.ds(pl.multiple_of(xs[d] * 256, 256), 256) for d in DELTAS}
    kept["wo"] = [local(wo_ref, w_out.at[q, c, :, x_columns[0]], 10)]

    barrier = pltpu.get_barrier_semaphore()
    peers = [partner, onward, behind] + [ways[w] for w in ("A+", "A-", "B+", "B-")]
    for d in (1, -1, 2):
        peers += [at(q, c, xs[d]), at(q, 1 - c, xs[d])]
    for peer in peers:
        pl.semaphore_signal(barrier, inc=1, device_id=peer, device_id_type=MESH)
    pl.semaphore_wait(barrier, len(peers))

    swapped = {"wo": []}
    for i, (k, src, dst) in enumerate(swaps):
        start(f"swap{i}", src.at[:, other_columns], dst, "p")
        swapped.setdefault(k, []).append(f"swap{i}")

    def slab(core, column):
        return pl.ds(pl.multiple_of(core * 128 + column * PIECE, PIECE), PIECE)

    halves = (pl.ds(0, 3), pl.ds(3, 3))

    def pass_on(key, half, d, way):
        ref = normed.at[halves[half], slab(c, xs[d]), :]
        start(key, ref, ref, way)

    def norm():
        load.wait()
        own_slab = slab(c, x)

        def one(i, _):
            wide = raw[i].astype(F32)
            mean = jnp.sum(wide * wide, axis=-1, keepdims=True) * (1.0 / WIDTH)
            scaled = wide * lax.rsqrt(mean + EPSILON)
            normed[i, own_slab, :] = (scaled * gain_ref[...]).astype(BF16)
            return 0

        lax.fori_loop(0, BATCH, one, 0)
        for half in range(2):
            pass_on(f"x+{half}", half, 0, "x+")
            pass_on(f"x-{1 - half}", 1 - half, 0, "x-")
            pass_on(f"p{half}", half, 0, "p")

    def token_step(needs, starts):
        def run():
            arrived(needs)
            for args in starts:
                pass_on(*args)

        return run

    tok.begin = norm
    tok.a = token_step("x+0", [("x++", 0, -1, "x+"), ("m-1.0", 0, -1, "p")])
    tok.b = token_step("x-1", [("x--", 1, 1, "x-"), ("m1.1", 1, 1, "p")])
    tok.c = token_step("x+1", [("m-1.1", 1, -1, "p")])
    tok.d = token_step("x-0", [("m1.0", 0, 1, "p")])
    tok.e = token_step("x++", [("m2.0", 0, 2, "p")])
    tok.f = token_step("x--", [("m2.1", 1, 2, "p")])

    def token_needs(d, half):
        if d == 0:
            return (f"p{half}",)
        if d == 2:
            return (("x++", "x--")[half], f"m2.{half}")
        return (("x-" if d == 1 else "x+") + str(half), f"m{d}.{half}")

    def block(k, da, db, half):
        chip = chip_of((a + da + 4) % 4, (b + db + 4) % 4)
        if k == "wo":
            rows = pl.ds(0, 64) if half is None else pl.ds(32 * half, 32)
            return w_out.at[chip, c, rows, x_columns[0]]
        if half is None:
            rows = pl.ds(pl.multiple_of(chip * 128, 128), 128)
        else:
            rows = pl.ds(pl.multiple_of(chip * 128 + 64 * half, 64), 64)
        return w_q.at[rows, :] if k == "q" else w_kv.at[int(k[2]), rows, :]

    def plane_step(k, name, needs, starts):
        def run():
            if name.endswith("begin"):
                for copy in kept[k]:
                    copy.wait()
                arrived(*swapped[k])
            arrived(*needs)
            for key, da, db, half, way in starts:
                ref = block(k, da, db, half)
                start(key, ref, ref, way)

        return run

    for k in ("kv2", "kv1", "kv0", "q", "wo"):
        for name, needs, starts in plane_tasks(k, LEAN[k]):
            setattr(parts[k], name.split(".")[1], plane_step(k, name, needs, starts))

    out_halves = (pl.ds(0, 8), pl.ds(8, 8), pl.ds(0, 16))

    def pass_out(key, half, d, way):
        ref = w_out.at[out_halves[half], c, :, x_columns[d]]
        start(key, ref, ref, way)

    def out_step(needs, starts):
        def run():
            arrived(*needs)
            for args in starts:
                pass_out(*args)

        return run

    out.begin = out_step((), [
        ("o+0", 0, 0, "x+"), ("o-1", 1, 0, "x-"), ("o+1", 1, 0, "x+"), ("o-0", 0, 0, "x-"), ("n0", 2, 0, "p")
    ])
    out.a = out_step(("o+0",), [("o++", 0, -1, "x+")])
    out.b = out_step(("o-1",), [("o--", 1, 1, "x-")])
    out.c = out_step(("o+0", "o+1"), [("n-1", 2, -1, "p")])
    out.d = out_step(("o-0", "o-1"), [("n1", 2, 1, "p")])
    out.e = out_step(("o++", "o--"), [("n2", 2, 2, "p")])

    def rows_of(d, part=pl.ds(0, BATCH)):
        pieces = [normed[part, slab(core, xs[d]), :] for core in range(2)]
        return jnp.concatenate([p.reshape(-1, WIDTH) for p in pieces], axis=0)

    def need_tokens(d):
        for half in range(2):
            arrived(*token_needs(d, half))

    def keep_kv(g, d, product, part=pl.ds(0, BATCH)):
        product = product.astype(BF16).reshape(2, -1, PIECE, 2 * HEAD)
        for core in range(2):
            first = pl.multiple_of(HALO[g] + core * 128 + xs[d] * PIECE, PIECE)
            kv[g][part, pl.ds(first, PIECE), :] = product[core]

    def at_wide(half, base, core, d):
        first = pl.multiple_of(base + core * 128 + xs[d] * PIECE, PIECE)
        return kv2.at[halves[half], pl.ds(first, PIECE), :]

    def project_wide(d, half):
        def run():
            arrived(*token_needs(d, half))
            part = halves[half]
            keep_kv(2, d, jnp.dot(rows_of(d, part), w_kv[2], preferred_element_type=F32), part)
            for core in (1, 0):
                start(f"w{core}{d}{half}", at_wide(half, 384, core, d), at_wide(half, 128, core, d), "h")

        return run

    def forward_wide(d, half):
        def run():
            arrived(f"w1{d}{half}")
            start(f"f{d}{half}", at_wide(half, 256, 0, d), at_wide(half, 0, 0, d), "h")

        return run

    near = send.prepare(kv0.at[:, pl.ds(ROWS, 32), :], kv0.at[:, pl.ds(0, 32), :], onward)
    middle = {}
    for d in DELTAS:
        to = pl.multiple_of(jnp.maximum(xs[d] - 1, 0) * PIECE, PIECE)
        own = pl.multiple_of(96 + 128 + jnp.maximum(xs[d], 1) * PIECE, PIECE)
        middle[d] = send.prepare(kv1.at[:, pl.ds(own, PIECE), :], kv1.at[:, pl.ds(to, PIECE), :], onward)

    def project_kv(g, d):
        def one(core, _):
            rows = normed[:, slab(core, xs[d]), :].reshape(BATCH * PIECE, WIDTH)
            product = jnp.dot(rows, w_kv[g], preferred_element_type=F32).astype(BF16)
            first = pl.multiple_of(HALO[g] + core * 128 + xs[d] * PIECE, PIECE)
            kv[g][:, pl.ds(first, PIECE), :] = product.reshape(BATCH, PIECE, 2 * HEAD)
            return 0

        def run():
            need_tokens(d)
            lax.fori_loop(0, 2, one, 0)
            if g == 1:
                pl.when(xs[d] > 0)(middle[d].start)
            else:
                pl.when(xs[d] == 3)(near.start)

        return run

    def project_q(d):
        def run():
            need_tokens(d)
            product = jnp.dot(rows_of(d), w_q[...], preferred_element_type=F32)
            product = product.astype(BF16).reshape(2, BATCH, PIECE, 3 * HEAD)
            for core in range(2):
                for g in range(3):
                    queries[g, :, slab(core, xs[d]), :] = product[core, :, :, g * HEAD : (g + 1) * HEAD]

        return run

    for d in DELTAS:
        for half in range(2):
            setattr(kv2_part, f"project{d % 4}{half}", project_wide(d, half))
            setattr(wide, f"onward{d % 4}{half}", forward_wide(d, half))
        setattr(kv1_part, f"project{d % 4}", project_kv(1, d))
        setattr(kv0_part, f"project{d % 4}", project_kv(0, d))
        setattr(q_part, f"project{d % 4}", project_q(d))

    def make_masks():
        own_logs[...] = jnp.zeros_like(own_logs)
        for half in range(2):
            row = 0
            for g in (2, 1, 0):
                key = lax.broadcasted_iota(jnp.int32, (SPAN[g], 128), 0)
                lane = lax.broadcasted_iota(jnp.int32, (SPAN[g], 128), 1)
                lag = lane - key + HALO[g]
                position = key + (half * 128 - HALO[g]) + q * ROWS
                met = (lag >= 0) & (lag <= STEPS * DILATION[g]) & (position >= 0)
                if DILATION[g] > 1:
                    met = met & ((lag & (DILATION[g] - 1)) == 0)
                bias[half, row : row + SPAN[g], :] = jnp.where(met, F32(0), F32(-1e30))
                row += SPAN[g]

    scale = 1.0 / math.sqrt(HEAD)
    column_of_mine = pl.ds(pl.multiple_of((2 * x + c) * HEAD, HEAD), HEAD)

    def attend(half, part):
        def one(i, _):
            parts, row = [], 0
            for g in (2, 1, 0):
                keys = kv[g][i, pl.ds(half * 128, SPAN[g]), pl.ds(0, HEAD)]
                query = queries[g, i, pl.ds(half * 128, 128), :]
                score = lax.dot_general(keys, query, NT, preferred_element_type=F32)
                parts.append(score * scale + bias[half, row : row + SPAN[g], :])
                row += SPAN[g]
            peak = functools.reduce(jnp.maximum, [jnp.max(p, axis=0, keepdims=True) for p in parts])
            total = jnp.zeros((1, 128), F32)
            mixture = jnp.zeros((HEAD, 128), F32)
            for g, part in zip((2, 1, 0), parts):
                lifted = jnp.exp(part - peak)
                total = total + jnp.sum(lifted, axis=0, keepdims=True)
                values = kv[g][i, pl.ds(half * 128, SPAN[g]), pl.ds(HEAD, HEAD)]
                mixture = mixture + lax.dot_general(
                    values, lifted.astype(BF16), TN, preferred_element_type=F32
                )
            own_logs[half, pl.ds(i, 1), :] = peak + jnp.log(total)
            heads[i, pl.ds(half * 128, 128), :] = (mixture / total).T.astype(BF16)
            return 0

        lax.fori_loop(3 * part, 3 * part + 3, one, 0, unroll=3)

    exchanged = []

    def exchange(half, part):
        for i, d in enumerate((2, 1, -1)):
            slot = EXCHANGE + 6 * part + 2 * i
            copy = pltpu.make_async_remote_copy(
                src_ref=heads.at[halves[part], slab(half, xs[d]), :],
                dst_ref=gathered.at[halves[part], :, column_of_mine],
                send_sem=send_sem.at[slot + half],
                recv_sem=recv_sem.at[slot + c],
                device_id=at(q, half, xs[d]),
                device_id_type=MESH,
            )
            copy.start()
            exchanged.append(copy)

    make_masks()
    order = (
        kv2_part.begin, tok.begin, kv1_part.begin, wo_part.begin, kv2_part.up, kv2_part.down,
        kv2_part.up0, kv1_part.up, kv1_part.down, kv1_part.up0, wo_part.up, wo_part.down,
        wo_part.up0, kv2_part.far, kv2_part.up3, kv1_part.far, kv2_part.down1, wo_part.far,
        kv1_part.up3, kv1_part.down1, wo_part.down1, kv0_part.begin, kv2_part.down2, wo_part.up3,
        tok.a, tok.b, kv1_part.down2, wo_part.down2, kv0_part.one, kv0_part.next0,
        kv2_part.finish, kv2_part.project00, kv2_part.project01, kv2_part.project30, kv0_part.two, kv1_part.finish,
        wo_part.finish, out.begin, kv1_part.project0, kv0_part.next1, kv2_part.project11, kv0_part.last0,
        wide.onward00, tok.c, tok.d, kv0_part.back, q_part.begin, kv0_part.next2,
        wide.onward01, kv0_part.last1, kv2_part.project31, kv1_part.project3, kv2_part.project10, kv1_part.project1,
        wide.onward30, kv0_part.next3, q_part.one, q_part.next0, kv0_part.last2, wide.onward11,
        tok.e, tok.f, kv0_part.last3, q_part.two, q_part.next1, kv2_part.project20,
        kv2_part.project21, q_part.last0, kv1_part.project2, wide.onward31, q_part.back, kv0_part.finish,
        kv0_part.project0, out.a, out.b, kv0_part.project1, q_part.next2, kv0_part.project3,
        wide.onward10, q_part.last1, kv0_part.project2, q_part.next3, q_part.last2, out.c,
        out.d, q_part.last3, wide.onward20, wide.onward21, q_part.finish, q_part.project0,
        q_part.project1, out.e, q_part.project3, q_part.project2,
    )
    for step in order:
        step()

    arrived(*(f"w{core}{d}{half}" for core in (1, 0) for d in DELTAS for half in range(2)))
    for d in DELTAS:
        pl.when(xs[d] > 0)(middle[d].wait_recv)
    near.wait_recv()
    for part in range(2):
        attend(1, part)
        exchange(1, part)
    arrived(*(f"f{d}{half}" for d in DELTAS for half in range(2)))
    for part in range(2):
        attend(0, part)
        exchange(0, part)
    start("logs", own_logs.at[1 - c], partner_logs, "p")
    start("heads", heads.at[:, slab(1 - c, x), :], gathered.at[:, :, column_of_mine], "p")
    stay = local(heads.at[:, slab(c, x), :], gathered.at[:, :, column_of_mine], 11)
    arrived("n0", "n1", "n-1", "n2", "logs")
    mine_logs, their_logs = own_logs[c], partner_logs[...]
    logs_ref[:, 0, :] = jnp.where(c == 0, mine_logs, their_logs)[:BATCH]
    logs_ref[:, 1, :] = jnp.where(c == 0, their_logs, mine_logs)[:BATCH]
    stay.wait()
    arrived("heads")
    for slot in range(12):
        pltpu.make_async_remote_copy(
            src_ref=heads.at[halves[0], pl.ds(0, PIECE), :],
            dst_ref=gathered.at[halves[slot // 6], :, column_of_mine],
            send_sem=send_sem.at[EXCHANGE + slot],
            recv_sem=recv_sem.at[EXCHANGE + slot],
            device_id=partner,
            device_id_type=MESH,
        ).wait_recv()

    combined = gathered[...].reshape(BATCH * PIECE, 8 * HEAD)

    def out_tile(i, _):
        tile = w_out[pl.ds(i * 4, 4)].reshape(512, 8 * HEAD)
        product = lax.dot_general(combined, tile, NT, preferred_element_type=F32)
        columns = pl.ds(pl.multiple_of(i * 512, 512), 512)
        mixed_ref[:, :, columns] = product.astype(BF16).reshape(BATCH, PIECE, 512)
        return 0

    lax.fori_loop(0, 4, out_tile, 0)
    for copy in send.started + exchanged + [near]:
        copy.wait_send()
    for d in DELTAS:
        pl.when(xs[d] > 0)(middle[d].wait_send)


def layer(tokens, norm_gain, w_query, w_key, w_value, w_out):
    any_space = pl.BlockSpec(memory_space=pl.ANY)
    vmem = pl.BlockSpec(memory_space=pltpu.VMEM)
    mixed, logs = pl.pallas_call(
        kernel,
        out_shape=(
            jax.ShapeDtypeStruct((BATCH, PIECE, WIDTH), BF16),
            jax.ShapeDtypeStruct((BATCH, 2, 128), F32),
        ),
        in_specs=[any_space, vmem, any_space, any_space, any_space, any_space],
        out_specs=(vmem, vmem),
        scratch_shapes=[
            pltpu.VMEM((BATCH, PIECE, WIDTH), BF16),
            pltpu.VMEM((BATCH, ROWS, WIDTH), BF16),
            pltpu.VMEM((3, WIDTH, 2 * HEAD), BF16),
            pltpu.VMEM((WIDTH, 3 * HEAD), BF16),
            pltpu.VMEM((16, 2, 64, 8 * HEAD), BF16),
            pltpu.VMEM((3, BATCH, ROWS, HEAD), BF16),
            pltpu.VMEM((BATCH, HALO[0] + ROWS, 2 * HEAD), BF16),
            pltpu.VMEM((BATCH, HALO[1] + ROWS, 2 * HEAD), BF16),
            pltpu.VMEM((BATCH, HALO[2] + ROWS, 2 * HEAD), BF16),
            pltpu.VMEM((2, sum(SPAN), 128), F32),
            pltpu.VMEM((BATCH, ROWS, HEAD), BF16),
            pltpu.VMEM((BATCH, PIECE, 8 * HEAD), BF16),
            pltpu.VMEM((2, 8, 128), F32),
            pltpu.VMEM((8, 128), F32),
            pltpu.SemaphoreType.DMA((COPIES,)),
            pltpu.SemaphoreType.DMA((COPIES,)),
            pltpu.SemaphoreType.DMA((12,)),
        ],
        compiler_params=pltpu.CompilerParams(
            collective_id=0, has_side_effects=True, vmem_limit_bytes=56 * 1024 * 1024
        ),
    )(
        jnp.transpose(tokens, (1, 0, 2)),
        norm_gain.reshape(1, WIDTH),
        w_query,
        w_key,
        w_value,
        jnp.transpose(w_out),
    )
    return jnp.transpose(mixed, (1, 0, 2)), jnp.transpose(logs, (2, 0, 1))


def solution(mesh):
    in_specs = (
        P(("sp", "tp"), None, None),
        P(),
        P(None, "sp", "tp"),
        P(None, "sp", "tp"),
        P(None, "sp", "tp"),
        P("tp", "sp"),
    )
    out_specs = (P(("sp", "tp"), None, None), P("sp", None, "tp"))
    return jax.shard_map(layer, mesh=mesh, in_specs=in_specs, out_specs=out_specs, check_vma=False)
```

```python
import functools
import math

import jax
import jax.numpy as jnp
from jax import lax
from jax.experimental import pallas as pl
from jax.experimental.pallas import tpu as pltpu
from jax.sharding import PartitionSpec as P

MESH = pl.DeviceIdType.MESH
BATCH = 6
WIDTH = 2048
HEAD = 128
STEPS = 24
EPSILON = 1e-06
ROWS = 256
PIECE = 32
HALO = (32, 96, 384)
SPAN = (160, 224, 512)
DILATION = (1, 4, 16)
COPIES = 216
EXCHANGE = 200
F32 = jnp.float32
BF16 = jnp.bfloat16
DELTAS = (0, 1, -1, 2)
LEAN = {"kv2": 0, "kv1": 0, "kv0": 2, "q": 2, "wo": 0}
NT = (((1,), (1,)), ((), ()))
TN = (((0,), (0,)), ((), ()))


class Steps:
    pass


class Sender:
    def __init__(self, send_sem, recv_sem):
        self.send_sem, self.recv_sem, self.started, self.count = send_sem, recv_sem, [], 0

    def __call__(self, src, dst, device):
        copy = self.prepare(src, dst, device)
        copy.start()
        self.started.append(copy)
        return copy

    def prepare(self, src, dst, device):
        slot = self.count
        self.count += 1
        return pltpu.make_async_remote_copy(
            src_ref=src,
            dst_ref=dst,
            send_sem=self.send_sem.at[slot],
            recv_sem=self.recv_sem.at[slot],
            device_id=device,
            device_id_type=MESH,
        )


def plane_tasks(k, lean):
    if lean == 0:
        tasks = [
            ("begin", (), [("A+", 0, 0, None, "A+"), ("A-", 0, 0, None, "A-"), ("B+0", 0, 0, None, "B+"), ("B-0", 0, 0, None, "B-")]),
            ("up", ("A+",), [("A++", -1, 0, 0, "A+"), ("B+-1", -1, 0, None, "B+"), ("B--1", -1, 0, None, "B-")]),
            ("down", ("A-",), [("A--", 1, 0, 1, "A-"), ("B+1", 1, 0, None, "B+"), ("B-1", 1, 0, None, "B-")]),
            ("far", ("A++", "A--"), [("B+2", 2, 0, None, "B+"), ("B-2", 2, 0, None, "B-")]),
            ("up0", ("B+0",), [("C0", 0, -1, None, "B+")]),
            ("up3", ("B+-1",), [("C-1", -1, -1, None, "B+")]),
            ("down1", ("B-1",), [("C1", 1, 1, None, "B-")]),
            ("down2", ("B-2",), [("C2", 2, 1, None, "B-")]),
            ("finish", ("B-0", "B--1", "B+1", "B+2", "C0", "C-1", "C1", "C2"), []),
        ]
    else:
        last = 1 if lean == 1 else None

        def spread(d):
            up = [(f"B+{d}", d, 0, 0, "B+")] if lean == 1 else []
            return [(f"B-{d}", d, 0, None, "B-"), *up]

        first_up = [("A+", 0, 0, 0, "A+")] if lean == 1 else []
        tasks = [
            ("begin", (), [("A-", 0, 0, None, "A-"), *first_up, *spread(0)]),
            ("one", ("A-",), [("A--", 1, 0, None, "A-"), *spread(1)]),
            ("two", ("A--",), [("A---", 2, 0, last, "A-"), *spread(2)]),
            ("back", ("A---", "A+")[: 3 - lean], spread(-1)),
        ]
        for d in DELTAS:
            tasks.append((f"next{d % 4}", (f"B-{d}",), [(f"C{d}", d, 1, None, "B-")]))
            tasks.append((f"last{d % 4}", (f"C{d}",), [(f"D{d}", d, 2, last, "B-")]))
        ends = ("D", "B+")[: 3 - lean]
        tasks.append(("finish", tuple(f"{w}{d}" for d in DELTAS for w in ends), []))
    return [
        (f"{k}.{n}", tuple(f"{k}.{w}" for w in needs), [(f"{k}.{key}", *rest) for key, *rest in starts])
        for n, needs, starts in tasks
    ]


def kernel(
    tokens_ref, gain_ref, wq_ref, wk_ref, wv_ref, wo_ref,
    mixed_ref, logs_ref,
    raw, normed, w_kv, w_q, w_out, queries, kv0, kv1, kv2, bias, heads, gathered,
    own_logs, partner_logs, send_sem, recv_sem, local_sem,
):
    s, x = lax.axis_index("sp"), lax.axis_index("tp")
    c, q = s % 2, s // 2
    y, z = q % 4, q // 4
    kv = (kv0, kv1, kv2)
    send = Sender(send_sem, recv_sem)
    tok, out, wide = Steps(), Steps(), Steps()
    kv2_part, kv1_part, kv0_part, q_part, wo_part = (Steps() for _ in range(5))
    parts = {"kv2": kv2_part, "kv1": kv1_part, "kv0": kv0_part, "q": q_part, "wo": wo_part}

    def at(chip, core, column):
        return (chip * 2 + core, column)

    def chip_of(a, b):
        return (1 - c) * (b * 4 + a) + c * (a * 4 + b)

    a, b = (1 - c) * y + c * z, (1 - c) * z + c * y
    xs = {d: (x + d + 4) % 4 for d in (0, 1, -1, 2)}
    partner = at(q, 1 - c, x)
    onward, behind = at((q + 1) % 16, c, x), at((q + 15) % 16, c, x)
    ways = {
        "A+": at(chip_of((a + 1) % 4, b), c, x),
        "A-": at(chip_of((a + 3) % 4, b), c, x),
        "B+": at(chip_of(a, (b + 1) % 4), c, x),
        "B-": at(chip_of(a, (b + 3) % 4), c, x),
        "x+": at(q, c, xs[1]),
        "x-": at(q, c, xs[-1]),
        "p": partner,
        "h": onward,
    }

    sent, seen = {}, set()

    def start(key, src, dst, way):
        sent[key] = send(src, dst, ways[way])

    def arrived(*keys):
        for key in keys:
            if key not in seen:
                seen.add(key)
                sent[key].wait_recv()

    def local(src, dst, slot):
        copy = pltpu.make_async_copy(src, dst, local_sem.at[slot])
        copy.start()
        return copy

    load = local(tokens_ref, raw, 0)
    mine = pl.ds(pl.multiple_of(q * 128 + c * 64, 64), 64)
    own_columns = pl.ds(pl.multiple_of(c * HEAD, HEAD), HEAD)
    other_columns = pl.ds(pl.multiple_of((1 - c) * HEAD, HEAD), HEAD)
    swaps = []
    for g in (2, 1, 0):
        for r, ref in enumerate((wk_ref, wv_ref)):
            swaps.append((f"kv{g}", ref.at[g], w_kv.at[g, mine, pl.ds(r * HEAD, HEAD)]))
    for g in range(3):
        swaps.append(("q", wq_ref.at[g], w_q.at[mine, pl.ds(g * HEAD, HEAD)]))
    kept = {}
    for i, (k, src, dst) in enumerate(swaps):
        kept.setdefault(k, []).append(local(src.at[:, own_columns], dst, 1 + i))
    x_columns = {d: pl.ds(pl.multiple_of(xs[d] * 256, 256), 256) for d in DELTAS}
    kept["wo"] = [local(wo_ref, w_out.at[q, c, :, x_columns[0]], 10)]

    barrier = pltpu.get_barrier_semaphore()
    peers = [partner, onward, behind] + [ways[w] for w in ("A+", "A-", "B+", "B-")]
    for d in (1, -1, 2):
        peers += [at(q, c, xs[d]), at(q, 1 - c, xs[d])]
    for peer in peers:
        pl.semaphore_signal(barrier, inc=1, device_id=peer, device_id_type=MESH)
    pl.semaphore_wait(barrier, len(peers))

    swapped = {"wo": []}
    for i, (k, src, dst) in enumerate(swaps):
        start(f"swap{i}", src.at[:, other_columns], dst, "p")
        swapped.setdefault(k, []).append(f"swap{i}")

    def slab(core, column):
        return pl.ds(pl.multiple_of(core * 128 + column * PIECE, PIECE), PIECE)

    halves = (pl.ds(0, 3), pl.ds(3, 3))

    def pass_on(key, half, d, way):
        ref = normed.at[halves[half], slab(c, xs[d]), :]
        start(key, ref, ref, way)

    def norm():
        load.wait()
        own_slab = slab(c, x)

        def one(i, _):
            wide = raw[i].astype(F32)
            mean = jnp.sum(wide * wide, axis=-1, keepdims=True) * (1.0 / WIDTH)
            scaled = wide * lax.rsqrt(mean + EPSILON)
            normed[i, own_slab, :] = (scaled * gain_ref[...]).astype(BF16)
            return 0

        lax.fori_loop(0, BATCH, one, 0)
        for half in range(2):
            pass_on(f"x+{half}", half, 0, "x+")
            pass_on(f"x-{1 - half}", 1 - half, 0, "x-")
            pass_on(f"p{half}", half, 0, "p")

    def token_step(needs, starts):
        def run():
            arrived(needs)
            for args in starts:
                pass_on(*args)

        return run

    tok.begin = norm
    tok.a = token_step("x+0", [("x++", 0, -1, "x+"), ("m-1.0", 0, -1, "p")])
    tok.b = token_step("x-1", [("x--", 1, 1, "x-"), ("m1.1", 1, 1, "p")])
    tok.c = token_step("x+1", [("m-1.1", 1, -1, "p")])
    tok.d = token_step("x-0", [("m1.0", 0, 1, "p")])
    tok.e = token_step("x++", [("m2.0", 0, 2, "p")])
    tok.f = token_step("x--", [("m2.1", 1, 2, "p")])

    def token_needs(d, half):
        if d == 0:
            return (f"p{half}",)
        if d == 2:
            return (("x++", "x--")[half], f"m2.{half}")
        return (("x-" if d == 1 else "x+") + str(half), f"m{d}.{half}")

    def block(k, da, db, half):
        chip = chip_of((a + da + 4) % 4, (b + db + 4) % 4)
        if k == "wo":
            rows = pl.ds(0, 64) if half is None else pl.ds(32 * half, 32)
            return w_out.at[chip, c, rows, x_columns[0]]
        if half is None:
            rows = pl.ds(pl.multiple_of(chip * 128, 128), 128)
        else:
            rows = pl.ds(pl.multiple_of(chip * 128 + 64 * half, 64), 64)
        return w_q.at[rows, :] if k == "q" else w_kv.at[int(k[2]), rows, :]

    def plane_step(k, name, needs, starts):
        def run():
            if name.endswith("begin"):
                for copy in kept[k]:
                    copy.wait()
                arrived(*swapped[k])
            arrived(*needs)
            for key, da, db, half, way in starts:
                ref = block(k, da, db, half)
                start(key, ref, ref, way)

        return run

    for k in ("kv2", "kv1", "kv0", "q", "wo"):
        for name, needs, starts in plane_tasks(k, LEAN[k]):
            setattr(parts[k], name.split(".")[1], plane_step(k, name, needs, starts))

    out_halves = (pl.ds(0, 8), pl.ds(8, 8), pl.ds(0, 16))

    def pass_out(key, half, d, way):
        ref = w_out.at[out_halves[half], c, :, x_columns[d]]
        start(key, ref, ref, way)

    def out_step(needs, starts):
        def run():
            arrived(*needs)
            for args in starts:
                pass_out(*args)

        return run

    out.begin = out_step((), [
        ("o+0", 0, 0, "x+"), ("o-1", 1, 0, "x-"), ("o+1", 1, 0, "x+"), ("o-0", 0, 0, "x-"), ("n0", 2, 0, "p")
    ])
    out.a = out_step(("o+0",), [("o++", 0, -1, "x+")])
    out.b = out_step(("o-1",), [("o--", 1, 1, "x-")])
    out.c = out_step(("o+0", "o+1"), [("n-1", 2, -1, "p")])
    out.d = out_step(("o-0", "o-1"), [("n1", 2, 1, "p")])
    out.e = out_step(("o++", "o--"), [("n2", 2, 2, "p")])

    def rows_of(d, part=pl.ds(0, BATCH)):
        pieces = [normed[part, slab(core, xs[d]), :] for core in range(2)]
        return jnp.concatenate([p.reshape(-1, WIDTH) for p in pieces], axis=0)

    def need_tokens(d):
        for half in range(2):
            arrived(*token_needs(d, half))

    def keep_kv(g, d, product, part=pl.ds(0, BATCH)):
        product = product.astype(BF16).reshape(2, -1, PIECE, 2 * HEAD)
        for core in range(2):
            first = pl.multiple_of(HALO[g] + core * 128 + xs[d] * PIECE, PIECE)
            kv[g][part, pl.ds(first, PIECE), :] = product[core]

    def at_wide(half, base, core, d):
        first = pl.multiple_of(base + core * 128 + xs[d] * PIECE, PIECE)
        return kv2.at[halves[half], pl.ds(first, PIECE), :]

    def project_wide(d, half):
        def run():
            arrived(*token_needs(d, half))
            part = halves[half]
            keep_kv(2, d, jnp.dot(rows_of(d, part), w_kv[2], preferred_element_type=F32), part)
            for core in (1, 0):
                start(f"w{core}{d}{half}", at_wide(half, 384, core, d), at_wide(half, 128, core, d), "h")

        return run

    def forward_wide(d, half):
        def run():
            arrived(f"w1{d}{half}")
            start(f"f{d}{half}", at_wide(half, 256, 0, d), at_wide(half, 0, 0, d), "h")

        return run

    near = send.prepare(kv0.at[:, pl.ds(ROWS, 32), :], kv0.at[:, pl.ds(0, 32), :], onward)
    middle = {}
    for d in DELTAS:
        to = pl.multiple_of(jnp.maximum(xs[d] - 1, 0) * PIECE, PIECE)
        own = pl.multiple_of(96 + 128 + jnp.maximum(xs[d], 1) * PIECE, PIECE)
        middle[d] = send.prepare(kv1.at[:, pl.ds(own, PIECE), :], kv1.at[:, pl.ds(to, PIECE), :], onward)

    def project_kv(g, d):
        def one(core, _):
            rows = normed[:, slab(core, xs[d]), :].reshape(BATCH * PIECE, WIDTH)
            product = jnp.dot(rows, w_kv[g], preferred_element_type=F32).astype(BF16)
            first = pl.multiple_of(HALO[g] + core * 128 + xs[d] * PIECE, PIECE)
            kv[g][:, pl.ds(first, PIECE), :] = product.reshape(BATCH, PIECE, 2 * HEAD)
            return 0

        def run():
            need_tokens(d)
            lax.fori_loop(0, 2, one, 0)
            if g == 1:
                pl.when(xs[d] > 0)(middle[d].start)
            else:
                pl.when(xs[d] == 3)(near.start)

        return run

    def project_q(d):
        def run():
            need_tokens(d)
            product = jnp.dot(rows_of(d), w_q[...], preferred_element_type=F32)
            product = product.astype(BF16).reshape(2, BATCH, PIECE, 3 * HEAD)
            for core in range(2):
                for g in range(3):
                    queries[g, :, slab(core, xs[d]), :] = product[core, :, :, g * HEAD : (g + 1) * HEAD]

        return run

    for d in DELTAS:
        for half in range(2):
            setattr(kv2_part, f"project{d % 4}{half}", project_wide(d, half))
            setattr(wide, f"onward{d % 4}{half}", forward_wide(d, half))
        setattr(kv1_part, f"project{d % 4}", project_kv(1, d))
        setattr(kv0_part, f"project{d % 4}", project_kv(0, d))
        setattr(q_part, f"project{d % 4}", project_q(d))

    def make_masks():
        own_logs[...] = jnp.zeros_like(own_logs)
        for half in range(2):
            row = 0
            for g in (2, 1, 0):
                key = lax.broadcasted_iota(jnp.int32, (SPAN[g], 128), 0)
                lane = lax.broadcasted_iota(jnp.int32, (SPAN[g], 128), 1)
                lag = lane - key + HALO[g]
                position = key + (half * 128 - HALO[g]) + q * ROWS
                met = (lag >= 0) & (lag <= STEPS * DILATION[g]) & (position >= 0)
                if DILATION[g] > 1:
                    met = met & ((lag & (DILATION[g] - 1)) == 0)
                bias[half, row : row + SPAN[g], :] = jnp.where(met, F32(0), F32(-1e30))
                row += SPAN[g]

    scale = 1.0 / math.sqrt(HEAD)
    column_of_mine = pl.ds(pl.multiple_of((2 * x + c) * HEAD, HEAD), HEAD)

    def attend(half, part):
        def one(i, _):
            parts, row = [], 0
            for g in (2, 1, 0):
                keys = kv[g][i, pl.ds(half * 128, SPAN[g]), pl.ds(0, HEAD)]
                query = queries[g, i, pl.ds(half * 128, 128), :]
                score = lax.dot_general(keys, query, NT, preferred_element_type=F32)
                parts.append(score * scale + bias[half, row : row + SPAN[g], :])
                row += SPAN[g]
            peak = functools.reduce(jnp.maximum, [jnp.max(p, axis=0, keepdims=True) for p in parts])
            total = jnp.zeros((1, 128), F32)
            mixture = jnp.zeros((HEAD, 128), F32)
            for g, part in zip((2, 1, 0), parts):
                lifted = jnp.exp(part - peak)
                total = total + jnp.sum(lifted, axis=0, keepdims=True)
                values = kv[g][i, pl.ds(half * 128, SPAN[g]), pl.ds(HEAD, HEAD)]
                mixture = mixture + lax.dot_general(
                    values, lifted.astype(BF16), TN, preferred_element_type=F32
                )
            own_logs[half, pl.ds(i, 1), :] = peak + jnp.log(total)
            heads[i, pl.ds(half * 128, 128), :] = (mixture / total).T.astype(BF16)
            return 0

        lax.fori_loop(3 * part, 3 * part + 3, one, 0, unroll=3)

    exchanged = []

    def exchange(half, part):
        for i, d in enumerate((2, 1, -1)):
            slot = EXCHANGE + 6 * part + 2 * i
            copy = pltpu.make_async_remote_copy(
                src_ref=heads.at[halves[part], slab(half, xs[d]), :],
                dst_ref=gathered.at[halves[part], :, column_of_mine],
                send_sem=send_sem.at[slot + half],
                recv_sem=recv_sem.at[slot + c],
                device_id=at(q, half, xs[d]),
                device_id_type=MESH,
            )
            copy.start()
            exchanged.append(copy)

    make_masks()
    order = (
        kv2_part.begin, tok.begin, kv1_part.begin, wo_part.begin, kv2_part.up, kv2_part.down,
        kv2_part.up0, kv1_part.up, kv1_part.down, kv1_part.up0, wo_part.up, wo_part.down,
        wo_part.up0, kv2_part.far, kv2_part.up3, kv1_part.far, kv2_part.down1, wo_part.far,
        kv1_part.up3, kv1_part.down1, wo_part.down1, kv0_part.begin, kv2_part.down2, wo_part.up3,
        tok.a, tok.b, kv1_part.down2, wo_part.down2, kv0_part.one, kv0_part.next0,
        kv2_part.finish, kv2_part.project00, kv2_part.project01, kv2_part.project30, kv0_part.two, kv1_part.finish,
        wo_part.finish, out.begin, kv1_part.project0, kv0_part.next1, kv2_part.project11, kv0_part.last0,
        wide.onward00, tok.c, tok.d, kv0_part.back, q_part.begin, kv0_part.next2,
        wide.onward01, kv0_part.last1, kv2_part.project31, kv1_part.project3, kv2_part.project10, kv1_part.project1,
        wide.onward30, kv0_part.next3, q_part.one, q_part.next0, kv0_part.last2, wide.onward11,
        tok.e, tok.f, kv0_part.last3, q_part.two, q_part.next1, kv2_part.project20,
        kv2_part.project21, q_part.last0, kv1_part.project2, wide.onward31, q_part.back, kv0_part.finish,
        kv0_part.project0, out.a, out.b, kv0_part.project1, q_part.next2, kv0_part.project3,
        wide.onward10, q_part.last1, kv0_part.project2, q_part.next3, q_part.last2, out.c,
        out.d, q_part.last3, wide.onward20, wide.onward21, q_part.finish, q_part.project0,
        q_part.project1, out.e, q_part.project3, q_part.project2,
    )
    for step in order:
        step()

    arrived(*(f"w{core}{d}{half}" for core in (1, 0) for d in DELTAS for half in range(2)))
    for d in DELTAS:
        pl.when(xs[d] > 0)(middle[d].wait_recv)
    near.wait_recv()
    for part in range(2):
        attend(1, part)
        exchange(1, part)
    arrived(*(f"f{d}{half}" for d in DELTAS for half in range(2)))
    for part in range(2):
        attend(0, part)
        exchange(0, part)
    start("logs", own_logs.at[1 - c], partner_logs, "p")
    start("heads", heads.at[:, slab(1 - c, x), :], gathered.at[:, :, column_of_mine], "p")
    stay = local(heads.at[:, slab(c, x), :], gathered.at[:, :, column_of_mine], 11)
    arrived("n0", "n1", "n-1", "n2", "logs")
    mine_logs, their_logs = own_logs[c], partner_logs[...]
    logs_ref[:, 0, :] = jnp.where(c == 0, mine_logs, their_logs)[:BATCH]
    logs_ref[:, 1, :] = jnp.where(c == 0, their_logs, mine_logs)[:BATCH]
    stay.wait()
    arrived("heads")
    for slot in range(12):
        pltpu.make_async_remote_copy(
            src_ref=heads.at[halves[0], pl.ds(0, PIECE), :],
            dst_ref=gathered.at[halves[slot // 6], :, column_of_mine],
            send_sem=send_sem.at[EXCHANGE + slot],
            recv_sem=recv_sem.at[EXCHANGE + slot],
            device_id=partner,
            device_id_type=MESH,
        ).wait_recv()

    combined = gathered[...].reshape(BATCH * PIECE, 8 * HEAD)

    def out_tile(i, _):
        tile = w_out[pl.ds(i * 4, 4)].reshape(512, 8 * HEAD)
        product = lax.dot_general(combined, tile, NT, preferred_element_type=F32)
        columns = pl.ds(pl.multiple_of(i * 512, 512), 512)
        mixed_ref[:, :, columns] = product.astype(BF16).reshape(BATCH, PIECE, 512)
        return 0

    lax.fori_loop(0, 4, out_tile, 0, unroll=4)
    for copy in send.started + exchanged + [near]:
        copy.wait_send()
    for d in DELTAS:
        pl.when(xs[d] > 0)(middle[d].wait_send)


def layer(tokens, norm_gain, w_query, w_key, w_value, w_out):
    any_space = pl.BlockSpec(memory_space=pl.ANY)
    vmem = pl.BlockSpec(memory_space=pltpu.VMEM)
    mixed, logs = pl.pallas_call(
        kernel,
        out_shape=(
            jax.ShapeDtypeStruct((BATCH, PIECE, WIDTH), BF16),
            jax.ShapeDtypeStruct((BATCH, 2, 128), F32),
        ),
        in_specs=[any_space, vmem, any_space, any_space, any_space, any_space],
        out_specs=(vmem, vmem),
        scratch_shapes=[
            pltpu.VMEM((BATCH, PIECE, WIDTH), BF16),
            pltpu.VMEM((BATCH, ROWS, WIDTH), BF16),
            pltpu.VMEM((3, WIDTH, 2 * HEAD), BF16),
            pltpu.VMEM((WIDTH, 3 * HEAD), BF16),
            pltpu.VMEM((16, 2, 64, 8 * HEAD), BF16),
            pltpu.VMEM((3, BATCH, ROWS, HEAD), BF16),
            pltpu.VMEM((BATCH, HALO[0] + ROWS, 2 * HEAD), BF16),
            pltpu.VMEM((BATCH, HALO[1] + ROWS, 2 * HEAD), BF16),
            pltpu.VMEM((BATCH, HALO[2] + ROWS, 2 * HEAD), BF16),
            pltpu.VMEM((2, sum(SPAN), 128), F32),
            pltpu.VMEM((BATCH, ROWS, HEAD), BF16),
            pltpu.VMEM((BATCH, PIECE, 8 * HEAD), BF16),
            pltpu.VMEM((2, 8, 128), F32),
            pltpu.VMEM((8, 128), F32),
            pltpu.SemaphoreType.DMA((COPIES,)),
            pltpu.SemaphoreType.DMA((COPIES,)),
            pltpu.SemaphoreType.DMA((12,)),
        ],
        compiler_params=pltpu.CompilerParams(
            collective_id=0, has_side_effects=True, vmem_limit_bytes=56 * 1024 * 1024
        ),
    )(
        jnp.transpose(tokens, (1, 0, 2)),
        norm_gain.reshape(1, WIDTH),
        w_query,
        w_key,
        w_value,
        jnp.transpose(w_out),
    )
    return jnp.transpose(mixed, (1, 0, 2)), jnp.transpose(logs, (2, 0, 1))


def solution(mesh):
    in_specs = (
        P(("sp", "tp"), None, None),
        P(),
        P(None, "sp", "tp"),
        P(None, "sp", "tp"),
        P(None, "sp", "tp"),
        P("tp", "sp"),
    )
    out_specs = (P(("sp", "tp"), None, None), P("sp", None, "tp"))
    return jax.shard_map(layer, mesh=mesh, in_specs=in_specs, out_specs=out_specs, check_vma=False)
```

```python
import functools
import math

import jax
import jax.numpy as jnp
from jax import lax
from jax.experimental import pallas as pl
from jax.experimental.pallas import tpu as pltpu
from jax.sharding import PartitionSpec as P

MESH = pl.DeviceIdType.MESH
BATCH = 6
WIDTH = 2048
HEAD = 128
STEPS = 24
EPSILON = 1e-06
ROWS = 256
PIECE = 32
HALO = (32, 96, 384)
SPAN = (160, 224, 512)
DILATION = (1, 4, 16)
COPIES = 216
EXCHANGE = 200
F32 = jnp.float32
BF16 = jnp.bfloat16
DELTAS = (0, 1, -1, 2)
LEAN = {"kv2": 0, "kv1": 0, "kv0": 2, "q": 2, "wo": 0}
NT = (((1,), (1,)), ((), ()))
TN = (((0,), (0,)), ((), ()))


class Steps:
    pass


class Sender:
    def __init__(self, send_sem, recv_sem):
        self.send_sem, self.recv_sem, self.started, self.count = send_sem, recv_sem, [], 0

    def __call__(self, src, dst, device):
        copy = self.prepare(src, dst, device)
        copy.start()
        self.started.append(copy)
        return copy

    def prepare(self, src, dst, device):
        slot = self.count
        self.count += 1
        return pltpu.make_async_remote_copy(
            src_ref=src,
            dst_ref=dst,
            send_sem=self.send_sem.at[slot],
            recv_sem=self.recv_sem.at[slot],
            device_id=device,
            device_id_type=MESH,
        )


def plane_tasks(k, lean):
    if lean == 0:
        tasks = [
            ("begin", (), [("A+", 0, 0, None, "A+"), ("A-", 0, 0, None, "A-"), ("B+0", 0, 0, None, "B+"), ("B-0", 0, 0, None, "B-")]),
            ("up", ("A+",), [("A++", -1, 0, 0, "A+"), ("B+-1", -1, 0, None, "B+"), ("B--1", -1, 0, None, "B-")]),
            ("down", ("A-",), [("A--", 1, 0, 1, "A-"), ("B+1", 1, 0, None, "B+"), ("B-1", 1, 0, None, "B-")]),
            ("far", ("A++", "A--"), [("B+2", 2, 0, None, "B+"), ("B-2", 2, 0, None, "B-")]),
            ("up0", ("B+0",), [("C0", 0, -1, None, "B+")]),
            ("up3", ("B+-1",), [("C-1", -1, -1, None, "B+")]),
            ("down1", ("B-1",), [("C1", 1, 1, None, "B-")]),
            ("down2", ("B-2",), [("C2", 2, 1, None, "B-")]),
            ("finish", ("B-0", "B--1", "B+1", "B+2", "C0", "C-1", "C1", "C2"), []),
        ]
    else:
        last = 1 if lean == 1 else None

        def spread(d):
            up = [(f"B+{d}", d, 0, 0, "B+")] if lean == 1 else []
            return [(f"B-{d}", d, 0, None, "B-"), *up]

        first_up = [("A+", 0, 0, 0, "A+")] if lean == 1 else []
        tasks = [
            ("begin", (), [("A-", 0, 0, None, "A-"), *first_up, *spread(0)]),
            ("one", ("A-",), [("A--", 1, 0, None, "A-"), *spread(1)]),
            ("two", ("A--",), [("A---", 2, 0, last, "A-"), *spread(2)]),
            ("back", ("A---", "A+")[: 3 - lean], spread(-1)),
        ]
        for d in DELTAS:
            tasks.append((f"next{d % 4}", (f"B-{d}",), [(f"C{d}", d, 1, None, "B-")]))
            tasks.append((f"last{d % 4}", (f"C{d}",), [(f"D{d}", d, 2, last, "B-")]))
        ends = ("D", "B+")[: 3 - lean]
        tasks.append(("finish", tuple(f"{w}{d}" for d in DELTAS for w in ends), []))
    return [
        (f"{k}.{n}", tuple(f"{k}.{w}" for w in needs), [(f"{k}.{key}", *rest) for key, *rest in starts])
        for n, needs, starts in tasks
    ]


def kernel(
    tokens_ref, gain_ref, wq_ref, wk_ref, wv_ref, wo_ref,
    mixed_ref, logs_ref,
    raw, normed, w_kv, w_q, w_out, queries, kv0, kv1, kv2, bias, heads, gathered,
    own_logs, partner_logs, send_sem, recv_sem, local_sem,
):
    s, x = lax.axis_index("sp"), lax.axis_index("tp")
    c, q = s % 2, s // 2
    y, z = q % 4, q // 4
    kv = (kv0, kv1, kv2)
    send = Sender(send_sem, recv_sem)
    tok, out, wide = Steps(), Steps(), Steps()
    kv2_part, kv1_part, kv0_part, q_part, wo_part = (Steps() for _ in range(5))
    parts = {"kv2": kv2_part, "kv1": kv1_part, "kv0": kv0_part, "q": q_part, "wo": wo_part}

    def at(chip, core, column):
        return (chip * 2 + core, column)

    def chip_of(a, b):
        return (1 - c) * (b * 4 + a) + c * (a * 4 + b)

    a, b = (1 - c) * y + c * z, (1 - c) * z + c * y
    xs = {d: (x + d + 4) % 4 for d in (0, 1, -1, 2)}
    partner = at(q, 1 - c, x)
    onward, behind = at((q + 1) % 16, c, x), at((q + 15) % 16, c, x)
    ways = {
        "A+": at(chip_of((a + 1) % 4, b), c, x),
        "A-": at(chip_of((a + 3) % 4, b), c, x),
        "B+": at(chip_of(a, (b + 1) % 4), c, x),
        "B-": at(chip_of(a, (b + 3) % 4), c, x),
        "x+": at(q, c, xs[1]),
        "x-": at(q, c, xs[-1]),
        "p": partner,
        "h": onward,
    }

    sent, seen = {}, set()

    def start(key, src, dst, way):
        sent[key] = send(src, dst, ways[way])

    def arrived(*keys):
        for key in keys:
            if key not in seen:
                seen.add(key)
                sent[key].wait_recv()

    def local(src, dst, slot):
        copy = pltpu.make_async_copy(src, dst, local_sem.at[slot])
        copy.start()
        return copy

    load = local(tokens_ref, raw, 0)
    mine = pl.ds(pl.multiple_of(q * 128 + c * 64, 64), 64)
    own_columns = pl.ds(pl.multiple_of(c * HEAD, HEAD), HEAD)
    other_columns = pl.ds(pl.multiple_of((1 - c) * HEAD, HEAD), HEAD)
    swaps = []
    for g in (2, 1, 0):
        for r, ref in enumerate((wk_ref, wv_ref)):
            swaps.append((f"kv{g}", ref.at[g], w_kv.at[g, mine, pl.ds(r * HEAD, HEAD)]))
    for g in range(3):
        swaps.append(("q", wq_ref.at[g], w_q.at[mine, pl.ds(g * HEAD, HEAD)]))
    kept = {}
    for i, (k, src, dst) in enumerate(swaps):
        kept.setdefault(k, []).append(local(src.at[:, own_columns], dst, 1 + i))
    x_columns = {d: pl.ds(pl.multiple_of(xs[d] * 256, 256), 256) for d in DELTAS}
    kept["wo"] = [local(wo_ref, w_out.at[q, c, :, x_columns[0]], 10)]

    barrier = pltpu.get_barrier_semaphore()
    peers = [partner, onward, behind] + [ways[w] for w in ("A+", "A-", "B+", "B-")]
    for d in (1, -1, 2):
        peers += [at(q, c, xs[d]), at(q, 1 - c, xs[d])]
    for peer in peers:
        pl.semaphore_signal(barrier, inc=1, device_id=peer, device_id_type=MESH)
    pl.semaphore_wait(barrier, len(peers))

    swapped = {"wo": []}
    for i, (k, src, dst) in enumerate(swaps):
        start(f"swap{i}", src.at[:, other_columns], dst, "p")
        swapped.setdefault(k, []).append(f"swap{i}")

    def slab(core, column):
        return pl.ds(pl.multiple_of(core * 128 + column * PIECE, PIECE), PIECE)

    halves = (pl.ds(0, 3), pl.ds(3, 3))

    def pass_on(key, half, d, way):
        ref = normed.at[halves[half], slab(c, xs[d]), :]
        start(key, ref, ref, way)

    def norm():
        load.wait()
        own_slab = slab(c, x)

        def one(i, _):
            wide = raw[i].astype(F32)
            mean = jnp.sum(wide * wide, axis=-1, keepdims=True) * (1.0 / WIDTH)
            scaled = wide * lax.rsqrt(mean + EPSILON)
            normed[i, own_slab, :] = (scaled * gain_ref[...]).astype(BF16)
            return 0

        lax.fori_loop(0, BATCH, one, 0, unroll=3)
        for half in range(2):
            pass_on(f"x+{half}", half, 0, "x+")
            pass_on(f"x-{1 - half}", 1 - half, 0, "x-")
            pass_on(f"p{half}", half, 0, "p")

    def token_step(needs, starts):
        def run():
            arrived(needs)
            for args in starts:
                pass_on(*args)

        return run

    tok.begin = norm
    tok.a = token_step("x+0", [("x++", 0, -1, "x+"), ("m-1.0", 0, -1, "p")])
    tok.b = token_step("x-1", [("x--", 1, 1, "x-"), ("m1.1", 1, 1, "p")])
    tok.c = token_step("x+1", [("m-1.1", 1, -1, "p")])
    tok.d = token_step("x-0", [("m1.0", 0, 1, "p")])
    tok.e = token_step("x++", [("m2.0", 0, 2, "p")])
    tok.f = token_step("x--", [("m2.1", 1, 2, "p")])

    def token_needs(d, half):
        if d == 0:
            return (f"p{half}",)
        if d == 2:
            return (("x++", "x--")[half], f"m2.{half}")
        return (("x-" if d == 1 else "x+") + str(half), f"m{d}.{half}")

    def block(k, da, db, half):
        chip = chip_of((a + da + 4) % 4, (b + db + 4) % 4)
        if k == "wo":
            rows = pl.ds(0, 64) if half is None else pl.ds(32 * half, 32)
            return w_out.at[chip, c, rows, x_columns[0]]
        if half is None:
            rows = pl.ds(pl.multiple_of(chip * 128, 128), 128)
        else:
            rows = pl.ds(pl.multiple_of(chip * 128 + 64 * half, 64), 64)
        return w_q.at[rows, :] if k == "q" else w_kv.at[int(k[2]), rows, :]

    def plane_step(k, name, needs, starts):
        def run():
            if name.endswith("begin"):
                for copy in kept[k]:
                    copy.wait()
                arrived(*swapped[k])
            arrived(*needs)
            for key, da, db, half, way in starts:
                ref = block(k, da, db, half)
                start(key, ref, ref, way)

        return run

    for k in ("kv2", "kv1", "kv0", "q", "wo"):
        for name, needs, starts in plane_tasks(k, LEAN[k]):
            setattr(parts[k], name.split(".")[1], plane_step(k, name, needs, starts))

    out_halves = (pl.ds(0, 8), pl.ds(8, 8), pl.ds(0, 16))

    def pass_out(key, half, d, way):
        ref = w_out.at[out_halves[half], c, :, x_columns[d]]
        start(key, ref, ref, way)

    def out_step(needs, starts):
        def run():
            arrived(*needs)
            for args in starts:
                pass_out(*args)

        return run

    out.begin = out_step((), [
        ("o+0", 0, 0, "x+"), ("o-1", 1, 0, "x-"), ("o+1", 1, 0, "x+"), ("o-0", 0, 0, "x-"), ("n0", 2, 0, "p")
    ])
    out.a = out_step(("o+0",), [("o++", 0, -1, "x+")])
    out.b = out_step(("o-1",), [("o--", 1, 1, "x-")])
    out.c = out_step(("o+0", "o+1"), [("n-1", 2, -1, "p")])
    out.d = out_step(("o-0", "o-1"), [("n1", 2, 1, "p")])
    out.e = out_step(("o++", "o--"), [("n2", 2, 2, "p")])

    def rows_of(d, part=pl.ds(0, BATCH)):
        pieces = [normed[part, slab(core, xs[d]), :] for core in range(2)]
        return jnp.concatenate([p.reshape(-1, WIDTH) for p in pieces], axis=0)

    def need_tokens(d):
        for half in range(2):
            arrived(*token_needs(d, half))

    def keep_kv(g, d, product, part=pl.ds(0, BATCH)):
        product = product.astype(BF16).reshape(2, -1, PIECE, 2 * HEAD)
        for core in range(2):
            first = pl.multiple_of(HALO[g] + core * 128 + xs[d] * PIECE, PIECE)
            kv[g][part, pl.ds(first, PIECE), :] = product[core]

    def at_wide(half, base, core, d):
        first = pl.multiple_of(base + core * 128 + xs[d] * PIECE, PIECE)
        return kv2.at[halves[half], pl.ds(first, PIECE), :]

    def project_wide(d, half):
        def run():
            arrived(*token_needs(d, half))
            part = halves[half]
            keep_kv(2, d, jnp.dot(rows_of(d, part), w_kv[2], preferred_element_type=F32), part)
            for core in (1, 0):
                start(f"w{core}{d}{half}", at_wide(half, 384, core, d), at_wide(half, 128, core, d), "h")

        return run

    def forward_wide(d, half):
        def run():
            arrived(f"w1{d}{half}")
            start(f"f{d}{half}", at_wide(half, 256, 0, d), at_wide(half, 0, 0, d), "h")

        return run

    near = send.prepare(kv0.at[:, pl.ds(ROWS, 32), :], kv0.at[:, pl.ds(0, 32), :], onward)
    middle = {}
    for d in DELTAS:
        to = pl.multiple_of(jnp.maximum(xs[d] - 1, 0) * PIECE, PIECE)
        own = pl.multiple_of(96 + 128 + jnp.maximum(xs[d], 1) * PIECE, PIECE)
        middle[d] = send.prepare(kv1.at[:, pl.ds(own, PIECE), :], kv1.at[:, pl.ds(to, PIECE), :], onward)

    def project_kv(g, d):
        def one(core, _):
            rows = normed[:, slab(core, xs[d]), :].reshape(BATCH * PIECE, WIDTH)
            product = jnp.dot(rows, w_kv[g], preferred_element_type=F32).astype(BF16)
            first = pl.multiple_of(HALO[g] + core * 128 + xs[d] * PIECE, PIECE)
            kv[g][:, pl.ds(first, PIECE), :] = product.reshape(BATCH, PIECE, 2 * HEAD)
            return 0

        def run():
            need_tokens(d)
            lax.fori_loop(0, 2, one, 0)
            if g == 1:
                pl.when(xs[d] > 0)(middle[d].start)
            else:
                pl.when(xs[d] == 3)(near.start)

        return run

    def project_q(d):
        def run():
            need_tokens(d)
            product = jnp.dot(rows_of(d), w_q[...], preferred_element_type=F32)
            product = product.astype(BF16).reshape(2, BATCH, PIECE, 3 * HEAD)
            for core in range(2):
                for g in range(3):
                    queries[g, :, slab(core, xs[d]), :] = product[core, :, :, g * HEAD : (g + 1) * HEAD]

        return run

    for d in DELTAS:
        for half in range(2):
            setattr(kv2_part, f"project{d % 4}{half}", project_wide(d, half))
            setattr(wide, f"onward{d % 4}{half}", forward_wide(d, half))
        setattr(kv1_part, f"project{d % 4}", project_kv(1, d))
        setattr(kv0_part, f"project{d % 4}", project_kv(0, d))
        setattr(q_part, f"project{d % 4}", project_q(d))

    def make_masks():
        own_logs[...] = jnp.zeros_like(own_logs)
        for half in range(2):
            row = 0
            for g in (2, 1, 0):
                key = lax.broadcasted_iota(jnp.int32, (SPAN[g], 128), 0)
                lane = lax.broadcasted_iota(jnp.int32, (SPAN[g], 128), 1)
                lag = lane - key + HALO[g]
                position = key + (half * 128 - HALO[g]) + q * ROWS
                met = (lag >= 0) & (lag <= STEPS * DILATION[g]) & (position >= 0)
                if DILATION[g] > 1:
                    met = met & ((lag & (DILATION[g] - 1)) == 0)
                bias[half, row : row + SPAN[g], :] = jnp.where(met, F32(0), F32(-1e30))
                row += SPAN[g]

    scale = 1.0 / math.sqrt(HEAD)
    column_of_mine = pl.ds(pl.multiple_of((2 * x + c) * HEAD, HEAD), HEAD)

    def attend(half, part):
        def one(i, _):
            parts, row = [], 0
            for g in (2, 1, 0):
                keys = kv[g][i, pl.ds(half * 128, SPAN[g]), pl.ds(0, HEAD)]
                query = queries[g, i, pl.ds(half * 128, 128), :]
                score = lax.dot_general(keys, query, NT, preferred_element_type=F32)
                parts.append(score * scale + bias[half, row : row + SPAN[g], :])
                row += SPAN[g]
            peak = functools.reduce(jnp.maximum, [jnp.max(p, axis=0, keepdims=True) for p in parts])
            total = jnp.zeros((1, 128), F32)
            mixture = jnp.zeros((HEAD, 128), F32)
            for g, part in zip((2, 1, 0), parts):
                lifted = jnp.exp(part - peak)
                total = total + jnp.sum(lifted, axis=0, keepdims=True)
                values = kv[g][i, pl.ds(half * 128, SPAN[g]), pl.ds(HEAD, HEAD)]
                mixture = mixture + lax.dot_general(
                    values, lifted.astype(BF16), TN, preferred_element_type=F32
                )
            own_logs[half, pl.ds(i, 1), :] = peak + jnp.log(total)
            heads[i, pl.ds(half * 128, 128), :] = (mixture / total).T.astype(BF16)
            return 0

        lax.fori_loop(3 * part, 3 * part + 3, one, 0, unroll=3)

    exchanged = []

    def exchange(half, part):
        for i, d in enumerate((2, 1, -1)):
            slot = EXCHANGE + 6 * part + 2 * i
            copy = pltpu.make_async_remote_copy(
                src_ref=heads.at[halves[part], slab(half, xs[d]), :],
                dst_ref=gathered.at[halves[part], :, column_of_mine],
                send_sem=send_sem.at[slot + half],
                recv_sem=recv_sem.at[slot + c],
                device_id=at(q, half, xs[d]),
                device_id_type=MESH,
            )
            copy.start()
            exchanged.append(copy)

    make_masks()
    order = (
        kv2_part.begin, tok.begin, kv1_part.begin, wo_part.begin, kv2_part.up, kv2_part.down,
        kv2_part.up0, kv1_part.up, kv1_part.down, kv1_part.up0, wo_part.up, wo_part.down,
        wo_part.up0, kv2_part.far, kv2_part.up3, kv1_part.far, kv2_part.down1, wo_part.far,
        kv1_part.up3, kv1_part.down1, wo_part.down1, kv0_part.begin, kv2_part.down2, wo_part.up3,
        tok.a, tok.b, kv1_part.down2, wo_part.down2, kv0_part.one, kv0_part.next0,
        kv2_part.finish, kv2_part.project00, kv2_part.project01, kv2_part.project30, kv0_part.two, kv1_part.finish,
        wo_part.finish, out.begin, kv1_part.project0, kv0_part.next1, kv2_part.project11, kv0_part.last0,
        wide.onward00, tok.c, tok.d, kv0_part.back, q_part.begin, kv0_part.next2,
        wide.onward01, kv0_part.last1, kv2_part.project31, kv1_part.project3, kv2_part.project10, kv1_part.project1,
        wide.onward30, kv0_part.next3, q_part.one, q_part.next0, kv0_part.last2, wide.onward11,
        tok.e, tok.f, kv0_part.last3, q_part.two, q_part.next1, kv2_part.project20,
        kv2_part.project21, q_part.last0, kv1_part.project2, wide.onward31, q_part.back, kv0_part.finish,
        kv0_part.project0, out.a, out.b, kv0_part.project1, q_part.next2, kv0_part.project3,
        wide.onward10, q_part.last1, kv0_part.project2, q_part.next3, q_part.last2, out.c,
        out.d, q_part.last3, wide.onward20, wide.onward21, q_part.finish, q_part.project0,
        q_part.project1, out.e, q_part.project3, q_part.project2,
    )
    for step in order:
        step()

    arrived(*(f"w{core}{d}{half}" for core in (1, 0) for d in DELTAS for half in range(2)))
    for d in DELTAS:
        pl.when(xs[d] > 0)(middle[d].wait_recv)
    near.wait_recv()
    for part in range(2):
        attend(1, part)
        exchange(1, part)
    arrived(*(f"f{d}{half}" for d in DELTAS for half in range(2)))
    for part in range(2):
        attend(0, part)
        exchange(0, part)
    start("logs", own_logs.at[1 - c], partner_logs, "p")
    start("heads", heads.at[:, slab(1 - c, x), :], gathered.at[:, :, column_of_mine], "p")
    stay = local(heads.at[:, slab(c, x), :], gathered.at[:, :, column_of_mine], 11)
    arrived("n0", "n1", "n-1", "n2", "logs")
    mine_logs, their_logs = own_logs[c], partner_logs[...]
    logs_ref[:, 0, :] = jnp.where(c == 0, mine_logs, their_logs)[:BATCH]
    logs_ref[:, 1, :] = jnp.where(c == 0, their_logs, mine_logs)[:BATCH]
    stay.wait()
    arrived("heads")
    for slot in range(12):
        pltpu.make_async_remote_copy(
            src_ref=heads.at[halves[0], pl.ds(0, PIECE), :],
            dst_ref=gathered.at[halves[slot // 6], :, column_of_mine],
            send_sem=send_sem.at[EXCHANGE + slot],
            recv_sem=recv_sem.at[EXCHANGE + slot],
            device_id=partner,
            device_id_type=MESH,
        ).wait_recv()

    combined = gathered[...].reshape(BATCH * PIECE, 8 * HEAD)

    def out_tile(i, _):
        tile = w_out[pl.ds(i * 4, 4)].reshape(512, 8 * HEAD)
        product = lax.dot_general(combined, tile, NT, preferred_element_type=F32)
        columns = pl.ds(pl.multiple_of(i * 512, 512), 512)
        mixed_ref[:, :, columns] = product.astype(BF16).reshape(BATCH, PIECE, 512)
        return 0

    lax.fori_loop(0, 4, out_tile, 0, unroll=4)
    for copy in send.started + exchanged + [near]:
        copy.wait_send()
    for d in DELTAS:
        pl.when(xs[d] > 0)(middle[d].wait_send)


def layer(tokens, norm_gain, w_query, w_key, w_value, w_out):
    any_space = pl.BlockSpec(memory_space=pl.ANY)
    vmem = pl.BlockSpec(memory_space=pltpu.VMEM)
    mixed, logs = pl.pallas_call(
        kernel,
        out_shape=(
            jax.ShapeDtypeStruct((BATCH, PIECE, WIDTH), BF16),
            jax.ShapeDtypeStruct((BATCH, 2, 128), F32),
        ),
        in_specs=[any_space, vmem, any_space, any_space, any_space, any_space],
        out_specs=(vmem, vmem),
        scratch_shapes=[
            pltpu.VMEM((BATCH, PIECE, WIDTH), BF16),
            pltpu.VMEM((BATCH, ROWS, WIDTH), BF16),
            pltpu.VMEM((3, WIDTH, 2 * HEAD), BF16),
            pltpu.VMEM((WIDTH, 3 * HEAD), BF16),
            pltpu.VMEM((16, 2, 64, 8 * HEAD), BF16),
            pltpu.VMEM((3, BATCH, ROWS, HEAD), BF16),
            pltpu.VMEM((BATCH, HALO[0] + ROWS, 2 * HEAD), BF16),
            pltpu.VMEM((BATCH, HALO[1] + ROWS, 2 * HEAD), BF16),
            pltpu.VMEM((BATCH, HALO[2] + ROWS, 2 * HEAD), BF16),
            pltpu.VMEM((2, sum(SPAN), 128), F32),
            pltpu.VMEM((BATCH, ROWS, HEAD), BF16),
            pltpu.VMEM((BATCH, PIECE, 8 * HEAD), BF16),
            pltpu.VMEM((2, 8, 128), F32),
            pltpu.VMEM((8, 128), F32),
            pltpu.SemaphoreType.DMA((COPIES,)),
            pltpu.SemaphoreType.DMA((COPIES,)),
            pltpu.SemaphoreType.DMA((12,)),
        ],
        compiler_params=pltpu.CompilerParams(
            collective_id=0, has_side_effects=True, vmem_limit_bytes=56 * 1024 * 1024
        ),
    )(
        jnp.transpose(tokens, (1, 0, 2)),
        norm_gain.reshape(1, WIDTH),
        w_query,
        w_key,
        w_value,
        jnp.transpose(w_out),
    )
    return jnp.transpose(mixed, (1, 0, 2)), jnp.transpose(logs, (2, 0, 1))


def solution(mesh):
    in_specs = (
        P(("sp", "tp"), None, None),
        P(),
        P(None, "sp", "tp"),
        P(None, "sp", "tp"),
        P(None, "sp", "tp"),
        P("tp", "sp"),
    )
    out_specs = (P(("sp", "tp"), None, None), P("sp", None, "tp"))
    return jax.shard_map(layer, mesh=mesh, in_specs=in_specs, out_specs=out_specs, check_vma=False)
```
